128 devices in a mesh: ep: 32 (over z, y, core), tp: 4 (over x).
Axes of the slice: x: 4, y: 4, z: 4, core: 2. Of those that a mesh axis runs over, the one named last changes fastest.
Arguments:
- tokens: bfloat16 [1536, 2048], P('ep'), may hold values from -6 to 6
- mix_gain: float32 [2048], replicated, may hold values from 0.1 to 1.9
- w_query: bfloat16 [2048, 1024], P(None, 'tp'), may hold values from -0.125 to 0.125
- w_key: bfloat16 [2048, 1024], P(None, 'tp'), may hold values from -0.125 to 0.125
- w_value: bfloat16 [2048, 1024], P(None, 'tp'), may hold values from -0.125 to 0.125
- w_outgate: bfloat16 [2048, 1024], P(None, 'tp'), may hold values from -0.125 to 0.125
- w_ingate: bfloat16 [2048, 8], P(None, 'tp'), may hold values from -0.125 to 0.125
- w_forget: bfloat16 [2048, 8], P(None, 'tp'), may hold values from -0.125 to 0.125
- in_bias: float32 [8], P('tp'), may hold values from -2 to 1
- forget_bias: float32 [8], P('tp'), may hold values from -1 to 4
- w_mix_out: bfloat16 [1024, 2048], replicated, may hold values from -0.1875 to 0.1875
- cell_state: float32 [1536, 8, 128, 128], P('ep', 'tp'), may hold values from -0.5 to 0.5
- norm_state: float32 [1536, 8, 128], P('ep', 'tp'), may hold values from -0.5 to 0.5
- max_state: float32 [1536, 8], P('ep', 'tp'), may hold values from -1 to 2
- moe_gain: float32 [2048], replicated, may hold values from 0.1 to 1.9
- route_ids: int32 [1536, 2], P('ep'), may hold values from 0 to 31, as said below
- route_weights: float32 [1536, 2], P('ep'), may hold values from 0.2 to 1
- expert_gate: bfloat16 [32, 2048, 1024], P('ep', None, 'tp'), may hold values from -0.125 to 0.125
- expert_up: bfloat16 [32, 2048, 1024], P('ep', None, 'tp'), may hold values from -0.125 to 0.125
- expert_down: bfloat16 [32, 1024, 2048], P('ep', 'tp'), may hold values from -0.1875 to 0.1875
- branch_gate: bfloat16 [2048], replicated, may hold values from -0.125 to 0.125
- dense_gate: bfloat16 [2048, 8192], P(None, ('ep', 'tp')), may hold values from -0.125 to 0.125
- dense_up: bfloat16 [2048, 8192], P(None, ('ep', 'tp')), may hold values from -0.125 to 0.125
- dense_down: bfloat16 [8192, 2048], P(('ep', 'tp')), may hold values from -0.25 to 0.25
Outputs:
- layer_out: bfloat16 [1536, 2048], P('ep', 'tp')
- new_cell: float32 [1536, 8, 128, 128], P('ep', 'tp')
- new_norm: float32 [1536, 8, 128], P('ep', 'tp')
- new_max: float32 [1536, 8], P('ep', 'tp')
The draws below stay inside these ranges and needn't reach their ends.
Inputs may be any that keep to these rules, and one draw needn't show every extreme that they name: `route_ids`: each row names two different experts of one group of 8 consecutive ids. Within the rows of one device no id appears more than 6 times, and some id appears exactly 6 times.
All inputs are finite; a program needn't handle non-finite values.
Results may differ from the reference program's by a relative error of at most 0.009.
The reference program's roundings to bfloat16 on the way count: a program that leaves them out, or rounds other values in their place, can miss the bound.
Values may be sent and summed in bfloat16 or wider, within the bound.
No kernel may reach another device: no remote copies, remote signals or barrier semaphores. Data moves between devices by JAX's collectives and lax.ppermute only.
A program may use at most 128 MiB of HBM per device.

```python
import jax
import jax.numpy as jnp
from jax import lax

D = 2048
HEADS = 8
HD = 128
EXP_FF = 1024
DFF = 8192
GROUPS = 4
TOPK = 2
SEQ_DEV = 48
EXPERTS = 32
EXPERTS_PER_GROUP = 8
SEQS = 1536
CAP = 6
N_EP = 32


def draw_route_ids(key, part):
    block_count = SEQS // SEQ_DEV
    rand_keys = jax.random.split(key, 4)
    full_group = jax.random.randint(rand_keys[0], (block_count, 1), 0, GROUPS)
    other_group = (full_group + 1 + jax.random.randint(rand_keys[1], (block_count, SEQ_DEV), 0, GROUPS - 1)) % GROUPS
    position = jnp.arange(SEQ_DEV, dtype=jnp.int32)[None, :]
    group_ids = jnp.where(position < CAP * EXPERTS_PER_GROUP // 2, full_group, other_group)
    shuffle = jax.vmap(lambda row_key: jax.random.permutation(row_key, SEQ_DEV))(jax.random.split(rand_keys[2], block_count))
    group_ids = jnp.take_along_axis(group_ids, shuffle, axis=1)
    one_hot = (group_ids[:, :, None] == jnp.arange(GROUPS, dtype=jnp.int32)[None, None, :]).astype(jnp.int32)
    slot_rank = jnp.sum((jnp.cumsum(one_hot, axis=1) - 1) * one_hot, axis=2)
    offsets = jax.random.randint(rand_keys[3], (block_count, GROUPS), 0, EXPERTS_PER_GROUP)
    start_expert = jnp.take_along_axis(offsets, group_ids, axis=1)
    first_pick = (start_expert + 2 * slot_rank) % EXPERTS_PER_GROUP
    second_pick = (first_pick + 1) % EXPERTS_PER_GROUP
    group_base = group_ids * EXPERTS_PER_GROUP
    picks = jnp.stack([group_base + first_pick, group_base + second_pick], axis=-1)
    return picks.reshape(SEQS, 2).astype(jnp.int32)


def raised(entries, rng, source, target, parts, factor):
    def block_of(dim):
        return (jnp.arange(entries.shape[dim]) // (entries.shape[dim] // parts)).reshape((-1,) + (1,) * (entries.ndim - 1 - dim))

    first = jax.random.permutation(rng, parts)[block_of(target)]
    second = (block_of(target) + parts // 2) % parts
    return jnp.where((block_of(source) == first) | (block_of(source) == second), factor * entries, entries)


def block_levels(key, extent, cuts, least, high):
    loudness = 1.0
    for dim, blocks in cuts:
        steps = jax.random.uniform(jax.random.fold_in(jax.random.fold_in(key, 6), dim), (blocks,), jnp.float32, least / len(cuts), high / len(cuts))
        loudness = loudness * jnp.repeat(jnp.exp(steps), extent[dim] // blocks).reshape((-1,) + (1,) * (len(extent) - 1 - dim))
    return loudness


def gaussian(key, dims, width, bound, shards=(), kind=jnp.bfloat16):
    entries = jax.random.normal(key, dims, jnp.float32) * width
    if len(shards) > 0:
        entries = block_levels(key, dims, shards, -0.22, 0.18) * entries
    return jnp.clip(entries, min=-bound, max=bound).astype(kind)


def gaussian_with(rng, dims, scale, reach, cuts, heavy, kind=jnp.bfloat16):
    values = scale * jax.random.normal(rng, dims, jnp.float32)
    if cuts:
        values = values * block_levels(rng, dims, cuts, -0.22, 0.18)
    return jnp.clip(raised(values, jax.random.fold_in(rng, 3), *heavy), -reach, reach).astype(kind)


def setup_inputs(seed: int = 0) -> dict:
    keys = jax.random.split(jax.random.key(seed), 25)
    return {
        "tokens": gaussian(keys[0], (SEQS, D), 1.0, 6.0, ((0, 32),)),
        "mix_gain": jnp.clip(1.0 + 0.18 * jax.random.normal(keys[1], (D,), jnp.float32), 0.1, 1.9),
        "w_query": gaussian(keys[2], (D, HEADS * HD), D ** -0.5, 0.125, ((1, 4),)),
        "w_key": gaussian(keys[3], (D, HEADS * HD), D ** -0.5, 0.125, ((1, 4),)),
        "w_value": gaussian(keys[4], (D, HEADS * HD), D ** -0.5, 0.125, ((1, 4),)),
        "w_outgate": gaussian(keys[5], (D, HEADS * HD), D ** -0.5, 0.125, ((1, 4),)),
        "w_ingate": gaussian(keys[6], (D, HEADS), D ** -0.5, 0.125, ((1, 4),)),
        "w_forget": gaussian(keys[7], (D, HEADS), D ** -0.5, 0.125, ((1, 4),)),
        "in_bias": jnp.clip(-2.0 + 3.0 * jax.random.uniform(keys[8], (HEADS,), jnp.float32) ** block_levels(keys[8], (HEADS,), ((0, 4),), -0.2, 0.2), -2.0, 1.0),
        "forget_bias": jnp.clip(-1.0 + 5.0 * jax.random.uniform(keys[9], (HEADS,), jnp.float32) ** block_levels(keys[9], (HEADS,), ((0, 4),), -0.2, 0.2), -1.0, 4.0),
        "w_mix_out": gaussian(keys[10], (HEADS * HD, D), (HEADS * HD) ** -0.5, 0.1875),
        "cell_state": gaussian(keys[11], (SEQS, HEADS, HD, HD), HD ** -0.5, 0.5, ((0, 32), (1, 4)), jnp.float32),
        "norm_state": gaussian(keys[12], (SEQS, HEADS, HD), HD ** -0.5, 0.5, ((0, 32), (1, 4)), jnp.float32),
        "max_state": jnp.clip(-1.0 + 3.0 * jax.random.uniform(keys[13], (SEQS, HEADS), jnp.float32) ** block_levels(keys[13], (SEQS, HEADS), ((0, 32), (1, 4)), -0.2, 0.2), -1.0, 2.0),
        "moe_gain": jnp.clip(1.0 + 0.18 * jax.random.normal(keys[14], (D,), jnp.float32), 0.1, 1.9),
        "route_ids": draw_route_ids(jax.random.fold_in(keys[24], 71), 0),
        "route_weights": jnp.clip(0.2 + 0.8 * jax.random.uniform(keys[16], (SEQS, TOPK), jnp.float32) ** block_levels(keys[16], (SEQS, TOPK), ((0, 32),), -0.2, 0.2), 0.2, 1.0),
        "expert_gate": gaussian(keys[17], (EXPERTS, D, EXP_FF), D ** -0.5, 0.125, ((0, 32), (2, 4))),
        "expert_up": gaussian(keys[18], (EXPERTS, D, EXP_FF), D ** -0.5, 0.125, ((0, 32), (2, 4))),
        "expert_down": gaussian(keys[19], (EXPERTS, EXP_FF, D), EXP_FF ** -0.5, 0.1875, ((0, 32), (1, 4))),
        "branch_gate": gaussian(keys[20], (D,), D ** -0.5, 0.125),
        "dense_gate": gaussian(keys[21], (D, DFF), D ** -0.5, 0.125, ((1, 128),)),
        "dense_up": gaussian(keys[22], (D, DFF), D ** -0.5, 0.125, ((1, 128),)),
        "dense_down": gaussian_with(keys[23], (DFF, D), DFF ** -0.5, 0.25, ((0, 128),), (0, 1, 128, 5.5)),
    }


EPS = 1e-06

def norm_rows(rows_in, gain_vec):
    as_float = rows_in.astype(jnp.float32)
    scaled = as_float * lax.rsqrt(lax.optimization_barrier(jnp.mean(as_float * as_float, axis=-1, keepdims=True)) + EPS)
    return (scaled * gain_vec).astype(jnp.bfloat16)

def swiglu(tok_rows, gate_w, up_w):
    gate_proj = jnp.dot(tok_rows, gate_w, preferred_element_type=jnp.float32)
    up_proj = jnp.dot(tok_rows, up_w, preferred_element_type=jnp.float32)
    return (jax.nn.silu(gate_proj) * up_proj).astype(jnp.bfloat16)

def cell_step(normed, w_query, w_key, w_value, w_outgate, w_ingate, w_forget, in_bias, forget_bias, cell_state, norm_state, max_state):
    row_count, head_count = max_state.shape
    head_size = cell_state.shape[2]

    def project(weight):
        return jnp.dot(normed, weight, preferred_element_type=jnp.float32)
    queries = project(w_query).reshape(row_count, head_count, head_size)
    key_vecs = project(w_key).reshape(row_count, head_count, head_size) * head_size ** (-0.5)
    values = project(w_value).reshape(row_count, head_count, head_size)
    outgate = project(w_outgate)
    in_pre = project(w_ingate) + in_bias
    log_forget = jax.nn.log_sigmoid(project(w_forget) + forget_bias)
    new_max = jnp.maximum(log_forget + max_state, in_pre)
    carry_factor = jnp.exp(log_forget + max_state - new_max)
    write_factor = jnp.exp(in_pre - new_max)
    written = write_factor[..., None] * key_vecs
    new_cell = carry_factor[..., None, None] * cell_state + written[..., :, None] * values[..., None, :]
    new_norm = carry_factor[..., None] * norm_state + written
    numerator = jnp.einsum('bhd,bhde->bhe', queries, new_cell, precision=lax.Precision.HIGHEST)
    denominator = lax.optimization_barrier(jnp.sum(queries * new_norm, axis=-1))
    cell_out = numerator / jnp.maximum(jnp.abs(denominator), jnp.exp(-new_max))[..., None]
    mixed_heads = (jax.nn.sigmoid(outgate) * cell_out.reshape(row_count, head_count * head_size)).astype(jnp.bfloat16)
    return (mixed_heads, new_cell, new_norm, new_max)

def reference(tokens, mix_gain, w_query, w_key, w_value, w_outgate, w_ingate, w_forget, in_bias, forget_bias, w_mix_out, cell_state, norm_state, max_state, moe_gain, route_ids, route_weights, expert_gate, expert_up, expert_down, branch_gate, dense_gate, dense_up, dense_down):
    normed = norm_rows(tokens, mix_gain)
    mixed_heads, new_cell, new_norm, new_max = cell_step(normed, w_query, w_key, w_value, w_outgate, w_ingate, w_forget, in_bias, forget_bias, cell_state, norm_state, max_state)
    mixed_proj = jnp.dot(mixed_heads, w_mix_out, preferred_element_type=jnp.float32)
    residual = (tokens.astype(jnp.float32) + mixed_proj).astype(jnp.bfloat16)
    moe_in = norm_rows(residual, moe_gain)
    flat_ids = route_ids.reshape(-1)
    owner_row = (jnp.arange(flat_ids.shape[0], dtype=jnp.int32) // route_ids.shape[1]).astype(jnp.int32)
    flat_weights = route_weights.reshape(-1)
    most_rows = N_EP * CAP

    def one_expert(total_out, inputs):
        expert_id, gate_w, up_w, down_w = inputs
        is_routed = flat_ids == expert_id
        slot_index = jnp.cumsum(is_routed.astype(jnp.int32)) - 1
        target = jnp.where(is_routed, slot_index, most_rows).astype(jnp.int32)
        row_index = jnp.zeros((most_rows,), jnp.int32).at[target].set(owner_row, mode='drop')
        slot_weight = jnp.zeros((most_rows,), jnp.float32).at[target].set(flat_weights, mode='drop')
        hidden = swiglu(moe_in[row_index], gate_w, up_w)
        expert_out = jnp.dot(hidden, down_w, preferred_element_type=jnp.float32) * slot_weight[:, None]
        return (total_out.at[row_index].add(expert_out), None)
    moe_out = lax.scan(one_expert, jnp.zeros((SEQS, D), jnp.float32), (jnp.arange(EXPERTS, dtype=jnp.int32), expert_gate, expert_up, expert_down))[0]
    dense_hidden = swiglu(moe_in, dense_gate, dense_up)
    branch_weight = jax.nn.sigmoid(jnp.dot(moe_in, branch_gate, preferred_element_type=jnp.float32))
    dense_out = branch_weight[:, None] * jnp.dot(dense_hidden, dense_down, preferred_element_type=jnp.float32)
    layer_out = (residual.astype(jnp.float32) + moe_out + dense_out).astype(jnp.bfloat16)
    return (layer_out, new_cell, new_norm, new_max)
```

```python
import jax
import jax.numpy as jnp
from jax import lax
from jax.experimental import pallas as pl
from jax.experimental.pallas import tpu as pltpu
from jax.sharding import Mesh
from jax.sharding import PartitionSpec as P


EPS = 1e-06
BF = jnp.bfloat16
F32 = jnp.float32
EP = ("q", "c")
ALL = ("q", "c", "x")
CORES = 2
VMEM = pl.BlockSpec(memory_space=pltpu.VMEM)
SMEM = pl.BlockSpec(memory_space=pltpu.SMEM)
ANY = pl.BlockSpec(memory_space=pl.ANY)


def params(mib=60):
    return pltpu.CompilerParams(vmem_limit_bytes=mib * 1024 * 1024)


def far_memory(array):
    return pltpu.with_memory_space_constraint(array, pltpu.HBM)


def near_memory(array):
    return pltpu.with_memory_space_constraint(array, pltpu.VMEM)


def nt_dot(left, right):
    return lax.dot_general(left, right, (((1,), (1,)), ((), ())), preferred_element_type=F32)


def normed_rows(rows_in, gain_vec):
    as_float = rows_in.astype(F32)
    mean = jnp.mean(as_float * as_float, axis=-1, keepdims=True)
    return (as_float * lax.rsqrt(mean + EPS) * gain_vec).astype(BF)


def log_sigmoid(x):
    return -(jnp.maximum(-x, 0.0) + jnp.log1p(jnp.exp(-jnp.abs(x))))


def gate_factors(in_pre, forget_pre, max_state):
    log_forget = log_sigmoid(forget_pre)
    new_max = jnp.maximum(log_forget + max_state, in_pre)
    return jnp.exp(log_forget + max_state - new_max), jnp.exp(in_pre - new_max), new_max


def padded_transpose(block):
    rows, cols = block.shape
    if rows < 128:
        block = jnp.concatenate([block, jnp.zeros((128 - rows, cols), block.dtype)], axis=0)
    return block.T


def front_kernel(
    tok, gain, wq, wk, wv, wo, w_in, w_fg, in_bias, fg_bias, cell, norm, mx,
    heads_o, carry_o, written_o, value_o, norm_o, max_o,
    wbuf, cbuf, num, wsem, csem,
):
    rows, head_count, hd = cbuf.shape[:3]
    chunks = csem.shape[0]
    per = rows // chunks
    weights = (wq, wk, wv, wo)
    loads = [pltpu.make_async_copy(w, wbuf.at[i], wsem.at[i]) for i, w in enumerate(weights)]
    parts = [
        pltpu.make_async_copy(cell.at[pl.ds(j * per, per)], cbuf.at[pl.ds(j * per, per)], csem.at[j])
        for j in range(chunks)
    ]
    for copy in loads + parts:
        copy.start()
    normed = normed_rows(tok[...], gain[...])
    in_row = nt_dot(w_in[...], normed)
    fg_row = nt_dot(w_fg[...], normed)
    factors = []
    for h in range(head_count):
        found = gate_factors(
            in_row[h : h + 1] + in_bias[h], fg_row[h : h + 1] + fg_bias[h], mx[h : h + 1]
        )
        max_o[h : h + 1] = found[2]
        factors += found
    factors.append(jnp.zeros((8 - len(factors), rows), F32))
    same = lax.broadcasted_iota(jnp.int32, (rows, rows), 0) == lax.broadcasted_iota(
        jnp.int32, (rows, rows), 1
    )
    columns = lax.dot_general(
        same.astype(F32),
        jnp.concatenate(factors, axis=0),
        (((1,), (1,)), ((), ())),
        preferred_element_type=F32,
        precision=lax.Precision.HIGHEST,
    )

    def project(i):
        loads[i].wait()
        return jnp.dot(normed, wbuf[i], preferred_element_type=F32)

    queries = project(0)
    keys = project(1) * hd ** (-0.5)
    values = project(2)
    outgate = project(3)
    turned = [padded_transpose(queries[:, h * hd : (h + 1) * hd]) for h in range(head_count)]
    for j in range(chunks):
        parts[j].wait()
        for b in range(j * per, (j + 1) * per):
            for h in range(head_count):
                num[h, b : b + 1] = jnp.sum(
                    turned[h][:, b : b + 1] * cbuf[b, h], axis=0, keepdims=True
                )
    for h in range(head_count):
        cols = slice(h * hd, (h + 1) * hd)
        carry, write, new_max = (columns[:, 3 * h + k : 3 * h + k + 1] for k in range(3))
        query, value = queries[:, cols], values[:, cols]
        written = write * keys[:, cols]
        at = pl.ds(h, rows, stride=head_count)
        new_norm = carry * norm[at, :] + written
        norm_o[at, :] = new_norm
        written_o[at, :] = written
        value_o[at, :] = value
        carry_o[at, :] = jnp.broadcast_to(carry, (rows, hd))
        numerator = carry * num[h] + jnp.sum(query * written, axis=-1, keepdims=True) * value
        denominator = jnp.sum(query * new_norm, axis=-1, keepdims=True)
        cell_out = numerator / jnp.maximum(jnp.abs(denominator), jnp.exp(-new_max))
        gated = (jax.nn.sigmoid(outgate[:, cols]) * cell_out).astype(BF)
        heads_o[:, cols] = gated


def update_kernel(carry, written, value, cell, out):
    turned = padded_transpose(written[...])
    for p in range(cell.shape[0]):
        out[p] = carry[p : p + 1] * cell[p] + turned[:, p : p + 1] * value[p : p + 1]


def over(index, divisor):
    factor, shift = {6: (10923, 16), 24: (43691, 20)}[divisor]
    return (index * factor) >> shift


def route_kernel(place, ids, select_o, slots_o):
    seqs = ids.shape[1]
    lanes = select_o.shape[1]
    row = lax.broadcasted_iota(jnp.int32, (seqs, seqs), 0)
    col = lax.broadcasted_iota(jnp.int32, (seqs, seqs), 1)
    first, second = ids[0:1], ids[1:2]
    here = lax.broadcasted_iota(jnp.int32, (seqs, lanes), 0)
    there = lax.broadcasted_iota(jnp.int32, (seqs, lanes), 1)
    slot_rows = []
    slots = jnp.zeros((seqs, lanes), jnp.int32)
    for k, own in enumerate((first, second)):
        column = jnp.sum(jnp.where(row == col, own, 0), axis=1, keepdims=True)
        same = ((column == first) | (column == second)) & (col < row)
        slot = column * 6 + jnp.sum(jnp.where(same, 1, 0), axis=1, keepdims=True)
        slots = jnp.where(there == k, slot, slots)
        slot_rows.append(
            jnp.sum(jnp.where((there & 63) == here, slot + 1, 0), axis=0, keepdims=True) - 1
        )
    slots_o[...] = slots
    size = select_o.shape[0]
    line = lax.broadcasted_iota(jnp.int32, (size, 1), 0)
    lane = lax.broadcasted_iota(jnp.int32, (1, lanes), 1)
    e = over(line, 24)
    inner = line - 24 * e
    part = over(inner, 6)
    entry = inner - 6 * part
    side, is_moe = part >> 1, part & 1
    dense_row = jnp.where(is_moe == 0, (place[0] * CORES + (e & 1)) * 6 + entry, -1)
    slot = jnp.where(is_moe == 1, e * 6 + entry, -2)
    hit = (dense_row == (lane & 63)) | (slot == slot_rows[0]) | (slot == slot_rows[1])
    select_o[...] = jnp.where(hit & (side == lane >> 6), 1.0, 0.0).astype(BF)


def plan_kernel(slots, picks_o, gather_o, spread_o):
    seqs = slots.shape[0]
    lanes = picks_o.shape[1]
    lane = lax.broadcasted_iota(jnp.int32, (1, lanes), 1)
    source = over(lane, 24)
    inner = lane - 24 * source
    part = over(inner, 6)
    entry = inner - 6 * part
    side, is_moe = part >> 1, part & 1
    from_x, from_c, from_e = source & 3, (source >> 2) & 1, source >> 2
    dense_row = jnp.where(is_moe == 0, (from_x * CORES + from_c) * 6 + entry, -1)
    slot = jnp.where(is_moe == 1, from_e * 6 + entry, -1)
    row = lax.broadcasted_iota(jnp.int32, (seqs, 1), 0)
    for k in range(3):
        if k == 0:
            hit = jnp.where(dense_row == row, 1.0, 0.0)
        else:
            hit = jnp.where(slot == slots[:, k - 1 : k], 1.0, 0.0)
        for h in range(2):
            at = (2 * k + h) * seqs
            picks_o[at : at + seqs] = jnp.where(side == h, hit, 0.0).astype(BF)
    size = gather_o.shape[0]
    col = lax.broadcasted_iota(jnp.int32, (1, size), 1)
    e = over(col, 24)
    inner = col - 24 * e
    part = over(inner, 6)
    grouped = part * (size // 4) + e * 6 + inner - 6 * part
    row = lax.broadcasted_iota(jnp.int32, (size, 1), 0)
    gather_o[...] = jnp.where(grouped == row, 1.0, 0.0).astype(BF)
    e = over(row, 24)
    inner = row - 24 * e
    part = over(inner, 6)
    grouped = part * (size // 4) + e * 6 + inner - 6 * part
    spread_o[...] = jnp.where(grouped == col, 1.0, 0.0).astype(BF)


def mix_kernel(
    place, heads, heads_l, heads_r, heads_f, w_mix, tok, gain, branch, select,
    send_o, own_o, weight_o,
    wbuf, sems,
):
    width = heads.shape[1]
    turns = (0, 3, 1, 2)
    loads = []
    for i, turn in enumerate(turns):
        start = pl.multiple_of(((place[0] + turn) & 3) * width, width)
        loads.append(pltpu.make_async_copy(w_mix.at[pl.ds(start, width)], wbuf.at[i], sems.at[i]))
        loads[i].start()
    mixed_proj = None
    for i, block in enumerate((heads, heads_l, heads_r, heads_f)):
        loads[i].wait()
        part = jnp.dot(block[...], wbuf[i], preferred_element_type=F32)
        mixed_proj = part if mixed_proj is None else mixed_proj + part
    residual = (tok[...].astype(F32) + mixed_proj).astype(BF)
    moe_in = normed_rows(residual, gain[...])
    half = send_o.shape[1]
    gap = jnp.zeros((select.shape[1] // 2 - moe_in.shape[0], half), BF)
    stacked = jnp.concatenate([moe_in[:, :half], gap, moe_in[:, half:], gap], axis=0)
    send_o[...] = jnp.dot(select[...], stacked, preferred_element_type=F32).astype(BF)
    cols = own_o.shape[1]
    own = residual[:, :cols]
    for k in range(1, residual.shape[1] // cols):
        own = jnp.where(place[0] == k, residual[:, k * cols : (k + 1) * cols], own)
    own_o[...] = own
    logit = jnp.sum(moe_in.astype(F32) * branch[...].astype(F32), axis=-1, keepdims=True)
    weight_o[...] = jnp.broadcast_to(jax.nn.sigmoid(logit), weight_o.shape)


def ffn_kernel(
    abuf, gather, spread, e_gate, e_up, e_down, *rest
):
    gates, boths = rest[:8], rest[8:16]
    out, gabuf, spbuf, egbuf, eubuf, edbuf, gbuf, ubuf, dbuf, xbuf, obuf, sems, osems = rest[16:]
    units = gates[0].shape[0]
    pairs = [
        (gather, gabuf), (e_gate, egbuf), (e_up, eubuf), (e_down, edbuf),
    ]
    for b in range(8):
        rows = pl.ds(b * units, units)
        pairs.append((gates[b], gbuf.at[rows]))
        pairs.append((boths[b].at[pl.ds(0, units)], ubuf.at[rows]))
        pairs.append((boths[b].at[pl.ds(units, units)], dbuf.at[rows]))
    pairs.append((spread, spbuf))
    loads = [pltpu.make_async_copy(src, dst, sems.at[i]) for i, (src, dst) in enumerate(pairs)]
    for copy in loads:
        copy.start()
    loads[0].wait()
    size, half = abuf.shape[0] // 4, abuf.shape[1]
    for part in range(4):
        piece = jnp.dot(
            gabuf[part * size : (part + 1) * size], abuf[...], preferred_element_type=F32
        )
        xbuf[part % 2, :, (part // 2) * half : (part // 2 + 1) * half] = piece.astype(BF)
    tok = xbuf[1]
    loads[1].wait()
    loads[2].wait()
    gate_proj = jnp.dot(tok, egbuf[0], preferred_element_type=F32)
    up_proj = jnp.dot(tok, eubuf[0], preferred_element_type=F32)
    hidden = (jax.nn.silu(gate_proj) * up_proj).astype(BF)
    loads[3].wait()
    expert_out = jnp.dot(hidden, edbuf[0], preferred_element_type=F32).astype(BF)
    tok = xbuf[0]
    total = None
    for side in range(2):
        for copy in loads[4 + 12 * side : 16 + 12 * side]:
            copy.wait()
        rows = slice(side * 4 * units, (side + 1) * 4 * units)
        hidden = (jax.nn.silu(nt_dot(tok, gbuf[rows])) * nt_dot(tok, ubuf[rows])).astype(BF)
        part = jnp.dot(hidden, dbuf[rows], preferred_element_type=F32)
        total = part if total is None else total + part
    total = total.astype(BF)
    loads[-1].wait()
    peers, quarter = obuf.shape[0], obuf.shape[3]
    stores = []
    for s in range(peers):
        sides = []
        for h in range(2):
            at = (2 * s + h) * quarter
            sides += [total[:, at : at + quarter], expert_out[:, at : at + quarter]]
        block = jnp.dot(spbuf[...], jnp.concatenate(sides, axis=0), preferred_element_type=F32)
        obuf[s] = block.reshape(obuf.shape[1:]).astype(BF)
        stores.append(pltpu.make_async_copy(obuf.at[s], out.at[:, s], osems.at[s]))
        stores[s].start()
    for copy in stores:
        copy.wait()


def final_kernel(picks, returned, own, weight, route_w, out):
    sums = jnp.dot(picks[...], returned[...], preferred_element_type=F32)
    seqs, quarter = own.shape[0], returned.shape[1]
    for h in range(2):
        dense, first, second = (
            sums[(2 * k + h) * seqs : (2 * k + h + 1) * seqs] for k in range(3)
        )
        cols = slice(h * quarter, (h + 1) * quarter)
        total = own[:, cols].astype(F32) + (route_w[:, :1] * first + route_w[:, 1:2] * second)
        out[:, cols] = (total + weight[:, :1] * dense).astype(BF)


def shape(*dims, dtype=F32):
    return jax.ShapeDtypeStruct(dims, dtype)


def local(
    tokens,
    mix_gain,
    w_query,
    w_key,
    w_value,
    w_outgate,
    w_ingate,
    w_forget,
    in_bias,
    forget_bias,
    w_mix_out,
    cell_state,
    norm_state,
    max_state,
    moe_gain,
    route_ids,
    route_weights,
    expert_gate,
    expert_up,
    expert_down,
    branch_gate,
    dense_gate,
    dense_up,
    dense_down,
):
    seqs, width = tokens.shape
    tp_count = lax.axis_size("x")
    chips = lax.axis_size("q")
    ep_count = chips * CORES
    place = lax.axis_index("x")
    cols = width // tp_count
    half = width // 2
    head_count, hd = cell_state.shape[1:3]
    pair_rows = seqs * head_count
    groups = tp_count * CORES
    share = seqs // groups
    capacity = max(2, 4 * seqs // ep_count)
    swap = [(0, 1), (1, 0)]

    right = [(i, (i + 1) % tp_count) for i in range(tp_count)]
    left = [(i, (i - 1) % tp_count) for i in range(tp_count)]
    across = [(i, (i + 2) % tp_count) for i in range(tp_count)]

    gate = dense_gate.T
    gate_l = lax.ppermute(gate, "x", right)
    gate_r = lax.ppermute(gate, "x", left)
    both = jnp.concatenate([dense_up.T, dense_down], axis=0)
    front_bytes = w_query.size * 4 * 2 + cell_state.size * 4
    heads, carry, written, value, new_norm, new_max = pl.pallas_call(
        front_kernel,
        in_specs=[VMEM, VMEM, ANY, ANY, ANY, ANY, VMEM, VMEM, SMEM, SMEM, ANY, VMEM, VMEM],
        out_specs=[VMEM] * 6,
        out_shape=[
            shape(seqs, head_count * hd, dtype=BF),
            shape(pair_rows, hd),
            shape(pair_rows, hd),
            shape(pair_rows, hd),
            shape(pair_rows, hd),
            shape(head_count, seqs),
        ],
        scratch_shapes=[
            pltpu.VMEM((4, *w_query.shape), BF),
            pltpu.VMEM(cell_state.shape, F32),
            pltpu.VMEM((head_count, seqs, hd), F32),
            pltpu.SemaphoreType.DMA((4,)),
            pltpu.SemaphoreType.DMA((6,)),
        ],
        compiler_params=params(),
        cost_estimate=pl.CostEstimate(
            flops=2 * seqs * width * 4 * head_count * hd, transcendentals=0, bytes_accessed=front_bytes
        ),
        name="front",
    )(
        tokens,
        mix_gain.reshape(1, width),
        far_memory(w_query),
        far_memory(w_key),
        far_memory(w_value),
        far_memory(w_outgate),
        w_ingate.T,
        w_forget.T,
        in_bias,
        forget_bias,
        far_memory(cell_state),
        norm_state.reshape(pair_rows, hd),
        max_state.T,
    )
    heads_l = lax.ppermute(heads, "x", right)
    heads_r = lax.ppermute(heads, "x", left)
    heads_f = lax.ppermute(heads, "x", across)
    both_l = lax.ppermute(both, "x", right)
    both_r = lax.ppermute(both, "x", left)
    gate_f = lax.ppermute(gate_l, "x", right)
    both_f = lax.ppermute(both_r, "x", left)
    gates, boths = [gate, gate_l, gate_r, gate_f], [both, both_l, both_r, both_f]
    gates += [lax.ppermute(w, "c", swap) for w in gates[:3]]
    boths += [lax.ppermute(w, "c", swap) for w in boths[:3]]
    gates.append(lax.ppermute(gate_f, "c", swap))
    boths.append(lax.ppermute(both_f, "c", swap))

    chunk_rows = 2 * (share + capacity)
    total_rows = ep_count * chunk_rows
    select, slots = pl.pallas_call(
        route_kernel,
        in_specs=[SMEM, VMEM],
        out_specs=[VMEM] * 2,
        out_shape=[
            shape(total_rows, 128, dtype=BF),
            shape(seqs, 128, dtype=jnp.int32),
        ],
        compiler_params=params(),
        name="route",
    )(place.reshape(1), route_ids.T)

    send, own, weight = pl.pallas_call(
        mix_kernel,
        in_specs=[SMEM] + [VMEM] * 4 + [ANY] + [VMEM] * 4,
        out_specs=[VMEM] * 3,
        out_shape=[
            pltpu.HBM((ep_count * chunk_rows, half), BF),
            shape(seqs, cols, dtype=BF),
            shape(seqs, 128),
        ],
        scratch_shapes=[
            pltpu.VMEM((tp_count, w_mix_out.shape[0] // tp_count, width), BF),
            pltpu.SemaphoreType.DMA((tp_count,)),
        ],
        compiler_params=params(40),
        cost_estimate=pl.CostEstimate(
            flops=2 * seqs * width * w_mix_out.shape[0], transcendentals=0, bytes_accessed=w_mix_out.size * 2
        ),
        name="mix",
    )(
        place.reshape(1),
        near_memory(heads),
        near_memory(heads_l),
        near_memory(heads_r),
        near_memory(heads_f),
        *(far_memory(a) for a in (w_mix_out, tokens, moe_gain.reshape(1, width))),
        *(far_memory(a) for a in (branch_gate.reshape(1, width), select)),
    )
    arrived = lax.all_to_all(
        send.reshape(ep_count, chunk_rows, half), EP, split_axis=0, concat_axis=0, tiled=True
    )
    sources = ep_count * tp_count
    quarter = cols // 2
    picks, gather, spread = pl.pallas_call(
        plan_kernel,
        in_specs=[VMEM],
        out_specs=[VMEM] * 3,
        out_shape=[
            pltpu.HBM((6 * seqs, sources * chunk_rows), BF),
            pltpu.HBM((total_rows, total_rows), BF),
            pltpu.HBM((total_rows, total_rows), BF),
        ],
        compiler_params=params(),
        name="plan",
    )(slots)
    many = ep_count * share
    units = gate.shape[0]
    back = pl.pallas_call(
        ffn_kernel,
        in_specs=[VMEM] + [ANY] * 21,
        out_specs=ANY,
        out_shape=pltpu.HBM((ep_count, tp_count, chunk_rows, quarter), BF),
        scratch_shapes=[
            pltpu.VMEM((total_rows, total_rows), BF),
            pltpu.VMEM((total_rows, total_rows), BF),
            pltpu.VMEM(expert_gate.shape, BF),
            pltpu.VMEM(expert_up.shape, BF),
            pltpu.VMEM(expert_down.shape, BF),
            pltpu.VMEM((8 * units, width), BF),
            pltpu.VMEM((8 * units, width), BF),
            pltpu.VMEM((8 * units, width), BF),
            pltpu.VMEM((2, many, width), BF),
            pltpu.VMEM((tp_count, ep_count, chunk_rows, quarter), BF),
            pltpu.SemaphoreType.DMA((29,)),
            pltpu.SemaphoreType.DMA((tp_count,)),
        ],
        compiler_params=params(46),
        cost_estimate=pl.CostEstimate(
            flops=6 * many * width * (8 * units + expert_down.shape[1]),
            transcendentals=0,
            bytes_accessed=6 * width * (8 * units + expert_down.shape[1]),
        ),
        name="ffn",
    )(near_memory(arrived.reshape(total_rows, half)), *(far_memory(a) for a in (
        gather, spread, expert_gate, expert_up, expert_down,
        *gates, *boths,
    )))
    returned = lax.all_to_all(
        back.reshape(sources, chunk_rows, quarter), ALL, split_axis=0, concat_axis=0, tiled=True
    )
    pairs = 16
    flat = pl.BlockSpec((pairs, hd), lambda i: (i, 0))
    cube = pl.BlockSpec((pairs, hd, hd), lambda i: (i, 0, 0))
    new_cell = pl.pallas_call(
        update_kernel,
        grid=(pair_rows // pairs,),
        in_specs=[flat, flat, flat, cube],
        out_specs=cube,
        out_shape=pltpu.HBM((pair_rows, hd, hd), F32),
        compiler_params=params(),
        cost_estimate=pl.CostEstimate(
            flops=3 * cell_state.size, transcendentals=0, bytes_accessed=8 * cell_state.size
        ),
        name="update",
    )(carry, written, value, far_memory(cell_state.reshape(pair_rows, hd, hd)))
    layer_out = pl.pallas_call(
        final_kernel,
        in_specs=[VMEM] * 5,
        out_specs=VMEM,
        out_shape=shape(seqs, cols, dtype=BF),
        compiler_params=params(40),
        name="final",
    )(
        far_memory(picks),
        near_memory(returned.reshape(sources * chunk_rows, quarter)),
        *(far_memory(a) for a in (own, weight, route_weights)),
    )
    return (
        layer_out,
        new_cell.reshape(cell_state.shape),
        new_norm.reshape(norm_state.shape),
        new_max.T,
    )


def solution(mesh):
    ep_count, tp_count = mesh.shape["ep"], mesh.shape["tp"]
    mesh = Mesh(mesh.devices.reshape(ep_count // CORES, CORES, tp_count), ALL)
    in_specs = (
        P(EP, None),
        P(),
        P(None, "x"),
        P(None, "x"),
        P(None, "x"),
        P(None, "x"),
        P(None, "x"),
        P(None, "x"),
        P("x"),
        P("x"),
        P(),
        P(EP, "x", None, None),
        P(EP, "x", None),
        P(EP, "x"),
        P(),
        P(EP, None),
        P(EP, None),
        P(EP, None, "x"),
        P(EP, None, "x"),
        P(EP, "x", None),
        P(),
        P(None, ALL),
        P(None, ALL),
        P(ALL, None),
    )
    out_specs = (P(EP, "x"), P(EP, "x", None, None), P(EP, "x", None), P(EP, "x"))
    return jax.shard_map(local, mesh=mesh, in_specs=in_specs, out_specs=out_specs, check_vma=False)
```

```python
import jax
import jax.numpy as jnp
from jax import lax
from jax.experimental import pallas as pl
from jax.experimental.pallas import tpu as pltpu
from jax.sharding import Mesh
from jax.sharding import PartitionSpec as P


EPS = 1e-06
BF = jnp.bfloat16
F32 = jnp.float32
EP = ("q", "c")
ALL = ("q", "c", "x")
CORES = 2
VMEM = pl.BlockSpec(memory_space=pltpu.VMEM)
SMEM = pl.BlockSpec(memory_space=pltpu.SMEM)
ANY = pl.BlockSpec(memory_space=pl.ANY)


def params(mib=60):
    return pltpu.CompilerParams(vmem_limit_bytes=mib * 1024 * 1024)


def far_memory(array):
    return pltpu.with_memory_space_constraint(array, pltpu.HBM)


def near_memory(array):
    return pltpu.with_memory_space_constraint(array, pltpu.VMEM)


def nt_dot(left, right):
    return lax.dot_general(left, right, (((1,), (1,)), ((), ())), preferred_element_type=F32)


def normed_rows(rows_in, gain_vec):
    as_float = rows_in.astype(F32)
    mean = jnp.mean(as_float * as_float, axis=-1, keepdims=True)
    return (as_float * lax.rsqrt(mean + EPS) * gain_vec).astype(BF)


def log_sigmoid(x):
    return -(jnp.maximum(-x, 0.0) + jnp.log1p(jnp.exp(-jnp.abs(x))))


def gate_factors(in_pre, forget_pre, max_state):
    log_forget = log_sigmoid(forget_pre)
    new_max = jnp.maximum(log_forget + max_state, in_pre)
    return jnp.exp(log_forget + max_state - new_max), jnp.exp(in_pre - new_max), new_max


def padded_transpose(block):
    rows, cols = block.shape
    if rows < 128:
        block = jnp.concatenate([block, jnp.zeros((128 - rows, cols), block.dtype)], axis=0)
    return block.T


def start_all(pairs, sems):
    copies = [pltpu.make_async_copy(src, dst, sems.at[i]) for i, (src, dst) in enumerate(pairs)]
    for copy in copies:
        copy.start()
    return copies


def over(index, divisor):
    factor, shift = {6: (10923, 16), 24: (43691, 20)}[divisor]
    return (index * factor) >> shift


def route_tables(place, ids, select_o, slots_o):
    seqs = ids.shape[1]
    lanes = select_o.shape[1]
    row = lax.broadcasted_iota(jnp.int32, (seqs, seqs), 0)
    col = lax.broadcasted_iota(jnp.int32, (seqs, seqs), 1)
    first, second = ids[0:1], ids[1:2]
    here = lax.broadcasted_iota(jnp.int32, (seqs, lanes), 0)
    there = lax.broadcasted_iota(jnp.int32, (seqs, lanes), 1)
    slot_rows = []
    slots = jnp.zeros((seqs, lanes), jnp.int32)
    for k, own in enumerate((first, second)):
        column = jnp.sum(jnp.where(row == col, own, 0), axis=1, keepdims=True)
        same = ((column == first) | (column == second)) & (col < row)
        slot = column * 6 + jnp.sum(jnp.where(same, 1, 0), axis=1, keepdims=True)
        slots = jnp.where(there == k, slot, slots)
        slot_rows.append(
            jnp.sum(jnp.where((there & 63) == here, slot + 1, 0), axis=0, keepdims=True) - 1
        )
    slots_o[...] = slots
    line = lax.broadcasted_iota(jnp.int32, (24, lanes), 0)
    lane = lax.broadcasted_iota(jnp.int32, (24, lanes), 1)
    part = over(line, 6)
    entry = line - 6 * part
    right_side = part >> 1 == lane >> 6
    is_moe = part & 1 == 1
    wanted = jnp.where(right_side & is_moe, entry, -999)
    shared = [
        right_side & (part & 1 == 0) & ((place * CORES + c) * 6 + entry == lane & 63)
        for c in range(CORES)
    ]
    for e in range(0, select_o.shape[0] // 24, 2):
        hits = []
        for c in range(2):
            first, second = (rows - 6 * (e + c) for rows in slot_rows)
            hit = shared[c] | (wanted == first) | (wanted == second)
            hits.append(jnp.where(hit, 1.0, 0.0))
        select_o[e * 24 : (e + 2) * 24] = jnp.concatenate(hits, axis=0).astype(BF)


def front_kernel(
    place, ids_h, tok_h, gain_h, w_in_h, w_fg_h, in_bias_h, fg_bias_h, norm_h, mx_h,
    wq, wk, wv, wo, cell, w_mix_h, moe_gain_h,
    heads_o, carry_h, written_h, value_h, norm_out_h, max_h, slots_h, select_o, w_mix, tok, moe_gain,
    ids, slots, gain, w_in, w_fg, in_bias, fg_bias, norm, mx, wbuf, cbuf, num,
    carry_o, written_o, value_o, norm_o, max_o, hot, isem, wsem, csem, osem,
):
    rows, head_count, hd = cbuf.shape[:3]
    chunks = csem.shape[0]
    per = rows // chunks
    small = start_all(
        [
            (tok_h, tok), (gain_h, gain), (w_in_h, w_in), (w_fg_h, w_fg),
            (in_bias_h, in_bias), (fg_bias_h, fg_bias), (norm_h, norm), (mx_h, mx),
            (ids_h, ids), (moe_gain_h, moe_gain),
        ],
        isem,
    )
    loads = [
        pltpu.make_async_copy(w, wbuf.at[i], wsem.at[i]) for i, w in enumerate((wq, wk, wv, wo))
    ]
    parts = [
        pltpu.make_async_copy(cell.at[pl.ds(j * per, per)], cbuf.at[pl.ds(j * per, per)], csem.at[j])
        for j in range(chunks)
    ]
    later = pltpu.make_async_copy(w_mix_h, w_mix, wsem.at[4])
    for copy in (loads[0], *parts, *loads[1:], later):
        copy.start()
    small[8].wait()
    route_tables(place[0], ids, select_o, slots)
    line = lax.broadcasted_iota(jnp.int32, hot.shape, 0) & 63
    hot[...] = jnp.where(line == lax.broadcasted_iota(jnp.int32, hot.shape, 1) >> 7, 1.0, 0.0).astype(BF)
    small[0].wait()
    small[1].wait()
    normed = normed_rows(tok[...], gain[...])
    for copy in small[2:8] + small[9:]:
        copy.wait()
    loads[0].wait()
    queries = jnp.dot(normed, wbuf[0], preferred_element_type=F32)
    high = queries.astype(BF).astype(F32)
    gap = jnp.zeros((64 - rows, head_count * hd), F32)
    stacked = jnp.concatenate([high, gap, queries - high, gap], axis=0)
    turned = jnp.concatenate(
        [stacked[:, h * hd : (h + 1) * hd].T for h in range(head_count)], axis=0
    ).astype(BF)

    def read_out(j):
        parts[j].wait()
        for b in range(j * per, (j + 1) * per, 2):
            spread = jnp.dot(turned, hot[:, b * hd : (b + 2) * hd], preferred_element_type=F32)
            for k in range(2):
                for h in range(head_count):
                    num[h, b + k : b + k + 1] = jnp.sum(
                        spread[h * hd : (h + 1) * hd, k * hd : (k + 1) * hd] * cbuf[b + k, h],
                        axis=0,
                        keepdims=True,
                    )

    read_out(0)
    in_row = nt_dot(w_in[...], normed)
    fg_row = nt_dot(w_fg[...], normed)
    factors = []
    for h in range(head_count):
        found = gate_factors(
            in_row[h : h + 1] + in_bias[h], fg_row[h : h + 1] + fg_bias[h], mx[h : h + 1]
        )
        max_o[h : h + 1] = found[2]
        factors += found
    factors.append(jnp.zeros((8 - len(factors), rows), F32))
    same = lax.broadcasted_iota(jnp.int32, (rows, rows), 0) == lax.broadcasted_iota(
        jnp.int32, (rows, rows), 1
    )
    columns = lax.dot_general(
        same.astype(F32),
        jnp.concatenate(factors, axis=0),
        (((1,), (1,)), ((), ())),
        preferred_element_type=F32,
        precision=lax.Precision.HIGHEST,
    )

    for j in range(1, chunks):
        read_out(j)

    def project(i):
        loads[i].wait()
        return jnp.dot(normed, wbuf[i], preferred_element_type=F32)

    keys = project(1) * hd ** (-0.5)
    values = project(2)
    kept = []
    for h in range(head_count):
        cols = slice(h * hd, (h + 1) * hd)
        carry, write, new_max = (columns[:, 3 * h + k : 3 * h + k + 1] for k in range(3))
        query, value = queries[:, cols], values[:, cols]
        written = write * keys[:, cols]
        at = pl.ds(h, rows, stride=head_count)
        new_norm = carry * norm[at, :] + written
        norm_o[at, :] = new_norm
        written_o[at, :] = written
        value_o[at, :] = value
        carry_o[at, :] = jnp.broadcast_to(carry, (rows, hd))
        denominator = jnp.sum(query * new_norm, axis=-1, keepdims=True)
        floor = jnp.maximum(jnp.abs(denominator), jnp.exp(-new_max))
        added = jnp.sum(query * written, axis=-1, keepdims=True) * value
        kept.append((carry, added, floor))
    stores = start_all(
        [
            (carry_o, carry_h), (written_o, written_h), (value_o, value_h),
            (norm_o, norm_out_h), (max_o, max_h), (slots, slots_h),
        ],
        osem,
    )
    opened = jax.nn.sigmoid(project(3))
    for h in range(head_count):
        cols = slice(h * hd, (h + 1) * hd)
        carry, added, floor = kept[h]
        heads_o[:, cols] = (opened[:, cols] * ((carry * num[h] + added) / floor)).astype(BF)
    for copy in stores:
        copy.wait()
    later.wait()


def update_kernel(carry, written, value, cell, out):
    turned = padded_transpose(written[...])
    for p in range(cell.shape[0]):
        out[p] = carry[p : p + 1] * cell[p] + turned[:, p : p + 1] * value[p : p + 1]


def plan_kernel(slots, moe_in, branch, picks_o, weight_o):
    logit = jnp.sum(moe_in[...].astype(F32) * branch[...].astype(F32), axis=-1, keepdims=True)
    weight_o[...] = jnp.broadcast_to(jax.nn.sigmoid(logit), weight_o.shape)
    seqs = slots.shape[0]
    lanes = picks_o.shape[1]
    lane = lax.broadcasted_iota(jnp.int32, (1, lanes), 1)
    source = over(lane, 24)
    inner = lane - 24 * source
    part = over(inner, 6)
    entry = inner - 6 * part
    side, is_moe = part >> 1, part & 1
    from_x, from_c, from_e = source & 3, (source >> 2) & 1, source >> 2
    dense_row = jnp.where(is_moe == 0, (from_x * CORES + from_c) * 6 + entry, -1)
    slot = jnp.where(is_moe == 1, from_e * 6 + entry, -1)
    row = lax.broadcasted_iota(jnp.int32, (seqs, 1), 0)
    for k in range(3):
        if k == 0:
            hit = jnp.where(dense_row == row, 1.0, 0.0)
        else:
            hit = jnp.where(slot == slots[:, k - 1 : k], 1.0, 0.0)
        for h in range(2):
            at = (2 * k + h) * seqs
            picks_o[at : at + seqs] = jnp.where(side == h, hit, 0.0).astype(BF)


def mix_kernel(
    place, heads, heads_l, heads_r, heads_f, w_mix, tok, gain, select,
    send_h, own_o, moe_o,
    send, sems,
):
    width = heads.shape[1]
    mixed_proj = None
    for turn, block in ((0, heads), (3, heads_l), (1, heads_r), (2, heads_f)):
        start = pl.multiple_of(((place[0] + turn) & 3) * width, width)
        part = jnp.dot(block[...], w_mix[pl.ds(start, width)], preferred_element_type=F32)
        mixed_proj = part if mixed_proj is None else mixed_proj + part
    residual = (tok[...].astype(F32) + mixed_proj).astype(BF)
    moe_in = normed_rows(residual, gain[...])
    half = send.shape[1]
    gap = jnp.zeros((select.shape[1] // 2 - moe_in.shape[0], half), BF)
    stacked = jnp.concatenate([moe_in[:, :half], gap, moe_in[:, half:], gap], axis=0)
    chunks = sems.shape[0]
    lines = send.shape[0] // chunks
    stores = []
    for j in range(chunks):
        at = pl.ds(j * lines, lines)
        send[at] = jnp.dot(select[at], stacked, preferred_element_type=F32).astype(BF)
        stores.append(pltpu.make_async_copy(send.at[at], send_h.at[at], sems.at[j]))
        stores[j].start()
    moe_o[...] = moe_in
    cols = own_o.shape[1]
    own = residual[:, :cols]
    for k in range(1, residual.shape[1] // cols):
        own = jnp.where(place[0] == k, residual[:, k * cols : (k + 1) * cols], own)
    own_o[...] = own
    for copy in stores:
        copy.wait()


def grouped_row(index, lines):
    source = over(index, 24)
    inner = index - 24 * source
    part = over(inner, 6)
    return part * lines + source * 6 + inner - 6 * part


def ffn_kernel(abuf, e_gate, e_up, e_down, *rest):
    packs, rest = rest[:10], rest[10:]
    out, egbuf, eubuf, edbuf, gbuf, ubuf, dbuf, xbuf, obuf, sems, osems = rest
    units = packs[0].shape[0] // 3
    mid = units // 2
    pairs = [(e_gate, egbuf), (e_up, eubuf), (e_down, edbuf)]
    for side in range(2):
        for b in range(3):
            pack, rows = packs[5 * side + b], pl.ds((4 * side + b) * units, units)
            pairs.append((pack.at[pl.ds(0, units)], gbuf.at[rows]))
            pairs.append((pack.at[pl.ds(units, units)], ubuf.at[rows]))
            pairs.append((pack.at[pl.ds(2 * units, units)], dbuf.at[rows]))
        head, tail, last = packs[5 * side + 3], packs[5 * side + 4], (4 * side + 3) * units
        pairs.append((head.at[pl.ds(0, units)], gbuf.at[pl.ds(last, units)]))
        pairs.append((head.at[pl.ds(units, mid)], ubuf.at[pl.ds(last, mid)]))
        pairs.append((tail.at[pl.ds(0, mid)], ubuf.at[pl.ds(last + mid, mid)]))
        pairs.append((tail.at[pl.ds(mid, units)], dbuf.at[pl.ds(last, units)]))
    loads = start_all(pairs, sems)
    size, half = abuf.shape
    block = 192
    groups = size // block
    lines = block // 4
    row = lax.broadcasted_iota(jnp.int32, (block, 1), 0)
    col = lax.broadcasted_iota(jnp.int32, (1, block), 1)
    gather = jnp.where(grouped_row(col, lines) == row, 1.0, 0.0).astype(BF)
    spread = jnp.where(grouped_row(row, lines) == col, 1.0, 0.0).astype(BF)
    for g in range(groups):
        sorted_rows = jnp.dot(
            gather, abuf[g * block : (g + 1) * block], preferred_element_type=F32
        ).astype(BF)
        for part in range(4):
            xbuf[
                part % 2,
                g * lines : (g + 1) * lines,
                (part // 2) * half : (part // 2 + 1) * half,
            ] = sorted_rows[part * lines : (part + 1) * lines]
    tok = xbuf[1]
    loads[0].wait()
    loads[1].wait()
    gate_proj = jnp.dot(tok, egbuf[0], preferred_element_type=F32)
    up_proj = jnp.dot(tok, eubuf[0], preferred_element_type=F32)
    hidden = (jax.nn.silu(gate_proj) * up_proj).astype(BF)
    loads[2].wait()
    expert_out = jnp.dot(hidden, edbuf[0], preferred_element_type=F32).astype(BF)
    tok = xbuf[0]
    total = None
    for side in range(2):
        for copy in loads[3 + 13 * side : 16 + 13 * side]:
            copy.wait()
        rows = slice(side * 4 * units, (side + 1) * 4 * units)
        hidden = (jax.nn.silu(nt_dot(tok, gbuf[rows])) * nt_dot(tok, ubuf[rows])).astype(BF)
        part = jnp.dot(hidden, dbuf[rows], preferred_element_type=F32)
        total = part if total is None else total + part
    total = total.astype(BF)
    peers, quarter = obuf.shape[0], obuf.shape[3]
    held = obuf.shape[1] // groups
    stores = []
    for s in range(peers):
        for g in range(groups):
            rows = slice(g * lines, (g + 1) * lines)
            sides = []
            for h in range(2):
                at = (2 * s + h) * quarter
                sides += [total[rows, at : at + quarter], expert_out[rows, at : at + quarter]]
            mixed = jnp.dot(spread, jnp.concatenate(sides, axis=0), preferred_element_type=F32)
            obuf[s, g * held : (g + 1) * held] = mixed.reshape(held, -1, quarter).astype(BF)
        stores.append(pltpu.make_async_copy(obuf.at[s], out.at[:, s], osems.at[s]))
        stores[s].start()
    for copy in stores:
        copy.wait()


def final_kernel(
    picks_h, returned, own_h, weight_h, route_h, out, picks, own, weight, route_w, sems
):
    loads = start_all(
        [(own_h, own), (weight_h, weight), (route_h, route_w), (picks_h, picks)], sems
    )
    for copy in loads:
        copy.wait()
    sums = jnp.dot(picks[...], returned[...], preferred_element_type=F32)
    seqs, quarter = own.shape[0], returned.shape[1]
    for h in range(2):
        dense, first, second = (
            sums[(2 * k + h) * seqs : (2 * k + h + 1) * seqs] for k in range(3)
        )
        cols = slice(h * quarter, (h + 1) * quarter)
        total = own[:, cols].astype(F32) + (route_w[:, :1] * first + route_w[:, 1:2] * second)
        out[:, cols] = (total + weight[:, :1] * dense).astype(BF)


def local(
    tokens,
    mix_gain,
    w_query,
    w_key,
    w_value,
    w_outgate,
    w_ingate,
    w_forget,
    in_bias,
    forget_bias,
    w_mix_out,
    cell_state,
    norm_state,
    max_state,
    moe_gain,
    route_ids,
    route_weights,
    expert_gate,
    expert_up,
    expert_down,
    branch_gate,
    dense_gate,
    dense_up,
    dense_down,
):
    seqs, width = tokens.shape
    tp_count = lax.axis_size("x")
    chips = lax.axis_size("q")
    ep_count = chips * CORES
    place = lax.axis_index("x")
    cols = width // tp_count
    half = width // 2
    head_count, hd = cell_state.shape[1:3]
    pair_rows = seqs * head_count
    groups = tp_count * CORES
    share = seqs // groups
    capacity = max(2, 4 * seqs // ep_count)
    swap = [(0, 1), (1, 0)]

    right = [(i, (i + 1) % tp_count) for i in range(tp_count)]
    left = [(i, (i - 1) % tp_count) for i in range(tp_count)]
    across = [(i, (i + 2) % tp_count) for i in range(tp_count)]

    top_count = route_ids.shape[1]
    chunk_rows = 2 * (share + capacity)
    total_rows = ep_count * chunk_rows
    pack = jnp.concatenate([dense_gate.T, dense_up.T, dense_down], axis=0)
    units = dense_down.shape[0]
    front_bytes = w_query.size * 4 * 2 + cell_state.size * 4
    (
        heads, carry, written, value, new_norm, new_max, slots, select, w_mix, tok, gain,
    ) = pl.pallas_call(
        front_kernel,
        in_specs=[SMEM] + [ANY] * 16,
        out_specs=[VMEM] + [ANY] * 6 + [VMEM] * 4,
        out_shape=[
            pltpu.VMEM((seqs, head_count * hd), BF),
            pltpu.HBM((pair_rows, hd), F32),
            pltpu.HBM((pair_rows, hd), F32),
            pltpu.HBM((pair_rows, hd), F32),
            pltpu.HBM((pair_rows, hd), F32),
            pltpu.HBM((head_count, seqs), F32),
            pltpu.HBM((seqs, 128), jnp.int32),
            pltpu.VMEM((total_rows, 128), BF),
            pltpu.VMEM(w_mix_out.shape, BF),
            pltpu.VMEM(tokens.shape, BF),
            pltpu.VMEM((1, width), F32),
        ],
        scratch_shapes=[
            pltpu.VMEM((top_count, seqs), jnp.int32),
            pltpu.VMEM((seqs, 128), jnp.int32),
            pltpu.VMEM((1, width), F32),
            pltpu.VMEM((head_count, width), BF),
            pltpu.VMEM((head_count, width), BF),
            pltpu.SMEM((head_count,), F32),
            pltpu.SMEM((head_count,), F32),
            pltpu.VMEM((pair_rows, hd), F32),
            pltpu.VMEM((head_count, seqs), F32),
            pltpu.VMEM((4, *w_query.shape), BF),
            pltpu.VMEM(cell_state.shape, F32),
            pltpu.VMEM((head_count, seqs, hd), F32),
            pltpu.VMEM((pair_rows, hd), F32),
            pltpu.VMEM((pair_rows, hd), F32),
            pltpu.VMEM((pair_rows, hd), F32),
            pltpu.VMEM((pair_rows, hd), F32),
            pltpu.VMEM((head_count, seqs), F32),
            pltpu.VMEM((128, seqs * hd), BF),
            pltpu.SemaphoreType.DMA((10,)),
            pltpu.SemaphoreType.DMA((5,)),
            pltpu.SemaphoreType.DMA((6,)),
            pltpu.SemaphoreType.DMA((6,)),
        ],
        compiler_params=params(40),
        cost_estimate=pl.CostEstimate(
            flops=2 * seqs * width * 4 * head_count * hd, transcendentals=0, bytes_accessed=front_bytes
        ),
        name="front",
    )(place.reshape(1), *(far_memory(a) for a in (
        route_ids.T,
        tokens,
        mix_gain.reshape(1, width),
        w_ingate.T,
        w_forget.T,
        in_bias,
        forget_bias,
        norm_state.reshape(pair_rows, hd),
        max_state.T,
        w_query,
        w_key,
        w_value,
        w_outgate,
        cell_state,
        w_mix_out,
        moe_gain.reshape(1, width),
    )))
    heads_l = lax.ppermute(heads, "x", right)
    heads_r = lax.ppermute(heads, "x", left)
    heads_f = lax.ppermute(heads, "x", across)
    pack_l = lax.ppermute(pack, "x", right)
    pack_r = lax.ppermute(pack, "x", left)
    cut = pack.shape[0] // 2
    head_f = lax.ppermute(pack_l[:cut], "x", right)
    tail_f = lax.ppermute(pack_r[cut:], "x", left)
    packs = [pack, pack_l, pack_r, head_f, tail_f]
    packs += [lax.ppermute(w, "c", swap) for w in packs]

    send, own, moe_in = pl.pallas_call(
        mix_kernel,
        in_specs=[SMEM] + [VMEM] * 8,
        out_specs=[ANY, VMEM, VMEM],
        out_shape=[
            pltpu.HBM((total_rows, half), BF),
            pltpu.HBM((seqs, cols), BF),
            pltpu.HBM((seqs, width), BF),
        ],
        scratch_shapes=[pltpu.VMEM((total_rows, half), BF), pltpu.SemaphoreType.DMA((4,))],
        compiler_params=params(30),
        cost_estimate=pl.CostEstimate(
            flops=2 * seqs * width * w_mix_out.shape[0], transcendentals=0, bytes_accessed=w_mix_out.size * 2
        ),
        name="mix",
    )(
        place.reshape(1),
        *(near_memory(a) for a in (heads, heads_l, heads_r, heads_f, w_mix, tok, gain, select)),
    )
    arrived = lax.all_to_all(
        send.reshape(ep_count, chunk_rows, half), EP, split_axis=0, concat_axis=0, tiled=True
    )
    sources = ep_count * tp_count
    quarter = cols // 2
    picks, weight = pl.pallas_call(
        plan_kernel,
        in_specs=[VMEM] * 3,
        out_specs=[VMEM] * 2,
        out_shape=[
            pltpu.HBM((6 * seqs, sources * chunk_rows), BF),
            pltpu.HBM((seqs, 128), F32),
        ],
        compiler_params=params(),
        name="plan",
    )(slots, moe_in, branch_gate.reshape(1, width))
    many = ep_count * share
    back = pl.pallas_call(
        ffn_kernel,
        in_specs=[VMEM] + [ANY] * 13,
        out_specs=ANY,
        out_shape=pltpu.HBM((ep_count, tp_count, chunk_rows, quarter), BF),
        scratch_shapes=[
            pltpu.VMEM(expert_gate.shape, BF),
            pltpu.VMEM(expert_up.shape, BF),
            pltpu.VMEM(expert_down.shape, BF),
            pltpu.VMEM((8 * units, width), BF),
            pltpu.VMEM((8 * units, width), BF),
            pltpu.VMEM((8 * units, width), BF),
            pltpu.VMEM((2, many, width), BF),
            pltpu.VMEM((tp_count, ep_count, chunk_rows, quarter), BF),
            pltpu.SemaphoreType.DMA((29,)),
            pltpu.SemaphoreType.DMA((tp_count,)),
        ],
        compiler_params=params(46),
        cost_estimate=pl.CostEstimate(
            flops=6 * many * width * (8 * units + expert_down.shape[1]),
            transcendentals=0,
            bytes_accessed=6 * width * (8 * units + expert_down.shape[1]),
        ),
        name="ffn",
    )(near_memory(arrived.reshape(total_rows, half)), *(far_memory(a) for a in (
        expert_gate, expert_up, expert_down,
        *packs,
    )))
    returned = lax.all_to_all(
        back.reshape(sources, chunk_rows, quarter), ALL, split_axis=0, concat_axis=0, tiled=True
    )
    pairs = 16
    flat = pl.BlockSpec((pairs, hd), lambda i: (i, 0))
    cube = pl.BlockSpec((pairs, hd, hd), lambda i: (i, 0, 0))
    new_cell = pl.pallas_call(
        update_kernel,
        grid=(pair_rows // pairs,),
        in_specs=[flat, flat, flat, cube],
        out_specs=cube,
        out_shape=pltpu.HBM((pair_rows, hd, hd), F32),
        compiler_params=params(),
        cost_estimate=pl.CostEstimate(
            flops=3 * cell_state.size, transcendentals=0, bytes_accessed=8 * cell_state.size
        ),
        name="update",
    )(carry, written, value, far_memory(cell_state.reshape(pair_rows, hd, hd)))
    layer_out = pl.pallas_call(
        final_kernel,
        in_specs=[ANY, VMEM, ANY, ANY, ANY],
        out_specs=VMEM,
        out_shape=pltpu.HBM((seqs, cols), BF),
        scratch_shapes=[
            pltpu.VMEM((6 * seqs, sources * chunk_rows), BF),
            pltpu.VMEM((seqs, cols), BF),
            pltpu.VMEM((seqs, 128), F32),
            pltpu.VMEM(route_weights.shape, F32),
            pltpu.SemaphoreType.DMA((4,)),
        ],
        compiler_params=params(40),
        name="final",
    )(
        far_memory(picks),
        near_memory(returned.reshape(sources * chunk_rows, quarter)),
        *(far_memory(a) for a in (own, weight, route_weights)),
    )
    return (
        layer_out,
        new_cell.reshape(cell_state.shape),
        new_norm.reshape(norm_state.shape),
        new_max.T,
    )


def solution(mesh):
    ep_count, tp_count = mesh.shape["ep"], mesh.shape["tp"]
    mesh = Mesh(mesh.devices.reshape(ep_count // CORES, CORES, tp_count), ALL)
    in_specs = (
        P(EP, None),
        P(),
        P(None, "x"),
        P(None, "x"),
        P(None, "x"),
        P(None, "x"),
        P(None, "x"),
        P(None, "x"),
        P("x"),
        P("x"),
        P(),
        P(EP, "x", None, None),
        P(EP, "x", None),
        P(EP, "x"),
        P(),
        P(EP, None),
        P(EP, None),
        P(EP, None, "x"),
        P(EP, None, "x"),
        P(EP, "x", None),
        P(),
        P(None, ALL),
        P(None, ALL),
        P(ALL, None),
    )
    out_specs = (P(EP, "x"), P(EP, "x", None, None), P(EP, "x", None), P(EP, "x"))
    return jax.shard_map(local, mesh=mesh, in_specs=in_specs, out_specs=out_specs, check_vma=False)
```

```python
import jax
import jax.numpy as jnp
from jax import lax
from jax.experimental import pallas as pl
from jax.experimental.pallas import tpu as pltpu
from jax.sharding import Mesh
from jax.sharding import PartitionSpec as P


EPS = 1e-06
BF = jnp.bfloat16
F32 = jnp.float32
EP = ("q", "c")
ALL = ("q", "c", "x")
CORES = 2
VMEM = pl.BlockSpec(memory_space=pltpu.VMEM)
SMEM = pl.BlockSpec(memory_space=pltpu.SMEM)
ANY = pl.BlockSpec(memory_space=pl.ANY)


def params(mib=60):
    return pltpu.CompilerParams(vmem_limit_bytes=mib * 1024 * 1024)


def far_memory(array):
    return pltpu.with_memory_space_constraint(array, pltpu.HBM)


def near_memory(array):
    return pltpu.with_memory_space_constraint(array, pltpu.VMEM)


def nt_dot(left, right):
    return lax.dot_general(left, right, (((1,), (1,)), ((), ())), preferred_element_type=F32)


def normed_rows(rows_in, gain_vec):
    as_float = rows_in.astype(F32)
    mean = jnp.mean(as_float * as_float, axis=-1, keepdims=True)
    return (as_float * lax.rsqrt(mean + EPS) * gain_vec).astype(BF)


def log_sigmoid(x):
    return -(jnp.maximum(-x, 0.0) + jnp.log1p(jnp.exp(-jnp.abs(x))))


def gate_factors(in_pre, forget_pre, max_state):
    log_forget = log_sigmoid(forget_pre)
    new_max = jnp.maximum(log_forget + max_state, in_pre)
    return jnp.exp(log_forget + max_state - new_max), jnp.exp(in_pre - new_max), new_max


def padded_transpose(block):
    rows, cols = block.shape
    if rows < 128:
        block = jnp.concatenate([block, jnp.zeros((128 - rows, cols), block.dtype)], axis=0)
    return block.T


def start_all(pairs, sems):
    copies = [pltpu.make_async_copy(src, dst, sems.at[i]) for i, (src, dst) in enumerate(pairs)]
    for copy in copies:
        copy.start()
    return copies


def over(index, divisor):
    factor, shift = {6: (10923, 16), 24: (43691, 20)}[divisor]
    return (index * factor) >> shift


def route_tables(place, ids, select_o, slots_o):
    seqs = ids.shape[1]
    lanes = select_o.shape[1]
    row = lax.broadcasted_iota(jnp.int32, (seqs, seqs), 0)
    col = lax.broadcasted_iota(jnp.int32, (seqs, seqs), 1)
    first, second = ids[0:1], ids[1:2]
    here = lax.broadcasted_iota(jnp.int32, (seqs, lanes), 0)
    there = lax.broadcasted_iota(jnp.int32, (seqs, lanes), 1)
    slot_rows = []
    slots = jnp.zeros((seqs, lanes), jnp.int32)
    for k, own in enumerate((first, second)):
        column = jnp.sum(jnp.where(row == col, own, 0), axis=1, keepdims=True)
        same = ((column == first) | (column == second)) & (col < row)
        slot = column * 6 + jnp.sum(jnp.where(same, 1, 0), axis=1, keepdims=True)
        slots = jnp.where(there == k, slot, slots)
        slot_rows.append(
            jnp.sum(jnp.where((there & 63) == here, slot + 1, 0), axis=0, keepdims=True) - 1
        )
    slots_o[...] = slots
    line = lax.broadcasted_iota(jnp.int32, (24, lanes), 0)
    lane = lax.broadcasted_iota(jnp.int32, (24, lanes), 1)
    part = over(line, 6)
    entry = line - 6 * part
    right_side = part >> 1 == lane >> 6
    is_moe = part & 1 == 1
    wanted = jnp.where(right_side & is_moe, entry, -999)
    shared = [
        right_side & (part & 1 == 0) & ((place * CORES + c) * 6 + entry == lane & 63)
        for c in range(CORES)
    ]
    for e in range(0, select_o.shape[0] // 24, 2):
        hits = []
        for c in range(2):
            first, second = (rows - 6 * (e + c) for rows in slot_rows)
            hit = shared[c] | (wanted == first) | (wanted == second)
            hits.append(jnp.where(hit, 1.0, 0.0))
        select_o[e * 24 : (e + 2) * 24] = jnp.concatenate(hits, axis=0).astype(BF)


def front_kernel(
    place, ids_h, tok_h, gain_h, w_in_h, w_fg_h, in_bias_h, fg_bias_h, norm_h, mx_h,
    wq, wk, wv, wo, cell, w_mix_h, moe_gain_h,
    heads_o, carry_h, written_h, value_h, norm_out_h, max_h, slots_h, select_o, w_mix, tok, moe_gain,
    ids, slots, gain, w_in, w_fg, in_bias, fg_bias, norm, mx, wbuf, cbuf, num,
    carry_o, written_o, value_o, norm_o, max_o, hot, isem, wsem, csem, osem,
):
    rows, head_count, hd = cbuf.shape[:3]
    chunks = csem.shape[0]
    per = rows // chunks
    small = start_all(
        [
            (tok_h, tok), (gain_h, gain), (w_in_h, w_in), (w_fg_h, w_fg),
            (in_bias_h, in_bias), (fg_bias_h, fg_bias), (norm_h, norm), (mx_h, mx),
            (ids_h, ids), (moe_gain_h, moe_gain),
        ],
        isem,
    )
    loads = [
        pltpu.make_async_copy(w, wbuf.at[i], wsem.at[i]) for i, w in enumerate((wq, wk, wv, wo))
    ]
    parts = [
        pltpu.make_async_copy(cell.at[pl.ds(j * per, per)], cbuf.at[pl.ds(j * per, per)], csem.at[j])
        for j in range(chunks)
    ]
    later = pltpu.make_async_copy(w_mix_h, w_mix, wsem.at[4])
    for copy in (loads[0], *parts, *loads[1:], later):
        copy.start()
    small[8].wait()
    route_tables(place[0], ids, select_o, slots)
    line = lax.broadcasted_iota(jnp.int32, hot.shape, 0) & 63
    hot[...] = jnp.where(line == lax.broadcasted_iota(jnp.int32, hot.shape, 1) >> 7, 1.0, 0.0).astype(BF)
    small[0].wait()
    small[1].wait()
    normed = normed_rows(tok[...], gain[...])
    for copy in small[2:8] + small[9:]:
        copy.wait()
    loads[0].wait()
    queries = jnp.dot(normed, wbuf[0], preferred_element_type=F32)
    high = queries.astype(BF).astype(F32)
    gap = jnp.zeros((64 - rows, head_count * hd), F32)
    stacked = jnp.concatenate([high, gap, queries - high, gap], axis=0)
    turned = jnp.concatenate(
        [stacked[:, h * hd : (h + 1) * hd].T for h in range(head_count)], axis=0
    ).astype(BF)

    def read_out(j):
        parts[j].wait()
        for b in range(j * per, (j + 1) * per, 2):
            spread = jnp.dot(turned, hot[:, b * hd : (b + 2) * hd], preferred_element_type=F32)
            for k in range(2):
                for h in range(head_count):
                    num[h, b + k : b + k + 1] = jnp.sum(
                        spread[h * hd : (h + 1) * hd, k * hd : (k + 1) * hd] * cbuf[b + k, h],
                        axis=0,
                        keepdims=True,
                    )

    read_out(0)
    in_row = nt_dot(w_in[...], normed)
    fg_row = nt_dot(w_fg[...], normed)
    factors = []
    for h in range(head_count):
        found = gate_factors(
            in_row[h : h + 1] + in_bias[h], fg_row[h : h + 1] + fg_bias[h], mx[h : h + 1]
        )
        max_o[h : h + 1] = found[2]
        factors += found
    factors.append(jnp.zeros((8 - len(factors), rows), F32))
    same = lax.broadcasted_iota(jnp.int32, (rows, rows), 0) == lax.broadcasted_iota(
        jnp.int32, (rows, rows), 1
    )
    columns = lax.dot_general(
        same.astype(F32),
        jnp.concatenate(factors, axis=0),
        (((1,), (1,)), ((), ())),
        preferred_element_type=F32,
        precision=lax.Precision.HIGHEST,
    )

    for j in range(1, chunks):
        read_out(j)

    def project(i):
        loads[i].wait()
        return jnp.dot(normed, wbuf[i], preferred_element_type=F32)

    keys = project(1) * hd ** (-0.5)
    values = project(2)
    kept = []
    for h in range(head_count):
        cols = slice(h * hd, (h + 1) * hd)
        carry, write, new_max = (columns[:, 3 * h + k : 3 * h + k + 1] for k in range(3))
        query, value = queries[:, cols], values[:, cols]
        written = write * keys[:, cols]
        at = pl.ds(h, rows, stride=head_count)
        new_norm = carry * norm[at, :] + written
        norm_o[at, :] = new_norm
        written_o[at, :] = written
        value_o[at, :] = value
        carry_o[at, :] = jnp.broadcast_to(carry, (rows, hd))
        denominator = jnp.sum(query * new_norm, axis=-1, keepdims=True)
        floor = jnp.maximum(jnp.abs(denominator), jnp.exp(-new_max))
        added = jnp.sum(query * written, axis=-1, keepdims=True) * value
        kept.append((carry, added, floor))
    stores = start_all(
        [
            (carry_o, carry_h), (written_o, written_h), (value_o, value_h),
            (norm_o, norm_out_h), (max_o, max_h), (slots, slots_h),
        ],
        osem,
    )
    opened = jax.nn.sigmoid(project(3))
    for h in range(head_count):
        cols = slice(h * hd, (h + 1) * hd)
        carry, added, floor = kept[h]
        heads_o[:, cols] = (opened[:, cols] * ((carry * num[h] + added) / floor)).astype(BF)
    for copy in stores:
        copy.wait()
    later.wait()


def update_kernel(carry, written, value, cell, out):
    turned = padded_transpose(written[...])
    for p in range(cell.shape[0]):
        out[p] = carry[p : p + 1] * cell[p] + turned[:, p : p + 1] * value[p : p + 1]


def plan_kernel(slots, moe_in, branch, picks_o, weight_o):
    logit = jnp.sum(moe_in[...].astype(F32) * branch[...].astype(F32), axis=-1, keepdims=True)
    weight_o[...] = jnp.broadcast_to(jax.nn.sigmoid(logit), weight_o.shape)
    seqs = slots.shape[0]
    lanes = picks_o.shape[1]
    lane = lax.broadcasted_iota(jnp.int32, (1, lanes), 1)
    source = over(lane, 24)
    inner = lane - 24 * source
    part = over(inner, 6)
    entry = inner - 6 * part
    side, is_moe = part >> 1, part & 1
    from_x, from_c, from_e = source & 3, (source >> 2) & 1, source >> 2
    dense_row = jnp.where(is_moe == 0, (from_x * CORES + from_c) * 6 + entry, -1)
    slot = jnp.where(is_moe == 1, from_e * 6 + entry, -1)
    row = lax.broadcasted_iota(jnp.int32, (seqs, 1), 0)
    for k in range(3):
        if k == 0:
            hit = jnp.where(dense_row == row, 1.0, 0.0)
        else:
            hit = jnp.where(slot == slots[:, k - 1 : k], 1.0, 0.0)
        for h in range(2):
            at = (2 * k + h) * seqs
            picks_o[at : at + seqs] = jnp.where(side == h, hit, 0.0).astype(BF)


def mix_kernel(
    place, heads, heads_l, heads_r, heads_f, w_mix, tok, gain, select,
    send_h, own_o, moe_o,
    send, sems,
):
    width = heads.shape[1]
    mixed_proj = None
    for turn, block in ((0, heads), (3, heads_l), (1, heads_r), (2, heads_f)):
        start = pl.multiple_of(((place[0] + turn) & 3) * width, width)
        part = jnp.dot(block[...], w_mix[pl.ds(start, width)], preferred_element_type=F32)
        mixed_proj = part if mixed_proj is None else mixed_proj + part
    residual = (tok[...].astype(F32) + mixed_proj).astype(BF)
    moe_in = normed_rows(residual, gain[...])
    half = send.shape[1]
    gap = jnp.zeros((select.shape[1] // 2 - moe_in.shape[0], half), BF)
    stacked = jnp.concatenate([moe_in[:, :half], gap, moe_in[:, half:], gap], axis=0)
    chunks = sems.shape[0]
    lines = send.shape[0] // chunks
    stores = []
    for j in range(chunks):
        at = pl.ds(j * lines, lines)
        send[at] = jnp.dot(select[at], stacked, preferred_element_type=F32).astype(BF)
        stores.append(pltpu.make_async_copy(send.at[at], send_h.at[at], sems.at[j]))
        stores[j].start()
    moe_o[...] = moe_in
    cols = own_o.shape[1]
    own = residual[:, :cols]
    for k in range(1, residual.shape[1] // cols):
        own = jnp.where(place[0] == k, residual[:, k * cols : (k + 1) * cols], own)
    own_o[...] = own
    for copy in stores:
        copy.wait()


def grouped_row(index, lines):
    source = over(index, 24)
    inner = index - 24 * source
    part = over(inner, 6)
    return part * lines + source * 6 + inner - 6 * part


def ffn_kernel(abuf, e_gate, e_up, e_down, *rest):
    packs, rest = rest[:8], rest[8:]
    out, egbuf, eubuf, edbuf, gbuf, ubuf, dbuf, xbuf, obuf, sems, osems = rest
    units = packs[0].shape[0] // 3
    pairs = []
    for b, pack in enumerate(packs):
        rows = pl.ds(b * units, units)
        pairs.append((pack.at[pl.ds(0, units)], gbuf.at[rows]))
        pairs.append((pack.at[pl.ds(units, units)], ubuf.at[rows]))
        pairs.append((pack.at[pl.ds(2 * units, units)], dbuf.at[rows]))
    pairs += [(e_gate, egbuf), (e_up, eubuf), (e_down, edbuf)]
    loads = start_all(pairs, sems)
    size, half = abuf.shape
    block = 192
    groups = size // block
    lines = block // 4
    row = lax.broadcasted_iota(jnp.int32, (block, 1), 0)
    col = lax.broadcasted_iota(jnp.int32, (1, block), 1)
    gather = jnp.where(grouped_row(col, lines) == row, 1.0, 0.0).astype(BF)
    spread = jnp.where(grouped_row(row, lines) == col, 1.0, 0.0).astype(BF)
    for g in range(groups):
        sorted_rows = jnp.dot(
            gather, abuf[g * block : (g + 1) * block], preferred_element_type=F32
        ).astype(BF)
        for part in range(4):
            xbuf[
                part % 2,
                g * lines : (g + 1) * lines,
                (part // 2) * half : (part // 2 + 1) * half,
            ] = sorted_rows[part * lines : (part + 1) * lines]
    tok = xbuf[0]
    total = None
    for side in range(2):
        for copy in loads[12 * side : 12 + 12 * side]:
            copy.wait()
        rows = slice(side * 4 * units, (side + 1) * 4 * units)
        hidden = (jax.nn.silu(nt_dot(tok, gbuf[rows])) * nt_dot(tok, ubuf[rows])).astype(BF)
        part = jnp.dot(hidden, dbuf[rows], preferred_element_type=F32)
        total = part if total is None else total + part
    total = total.astype(BF)
    tok = xbuf[1]
    loads[24].wait()
    loads[25].wait()
    gate_proj = jnp.dot(tok, egbuf[0], preferred_element_type=F32)
    up_proj = jnp.dot(tok, eubuf[0], preferred_element_type=F32)
    hidden = (jax.nn.silu(gate_proj) * up_proj).astype(BF)
    loads[26].wait()
    expert_out = jnp.dot(hidden, edbuf[0], preferred_element_type=F32).astype(BF)
    peers, quarter = obuf.shape[0], obuf.shape[3]
    held = obuf.shape[1] // groups
    stores = []
    for s in range(peers):
        for g in range(groups):
            rows = slice(g * lines, (g + 1) * lines)
            sides = []
            for h in range(2):
                at = (2 * s + h) * quarter
                sides += [total[rows, at : at + quarter], expert_out[rows, at : at + quarter]]
            mixed = jnp.dot(spread, jnp.concatenate(sides, axis=0), preferred_element_type=F32)
            obuf[s, g * held : (g + 1) * held] = mixed.reshape(held, -1, quarter).astype(BF)
        stores.append(pltpu.make_async_copy(obuf.at[s], out.at[:, s], osems.at[s]))
        stores[s].start()
    for copy in stores:
        copy.wait()


def final_kernel(
    picks_h, returned, own_h, weight_h, route_h, out, picks, own, weight, route_w, sems
):
    loads = start_all(
        [(own_h, own), (weight_h, weight), (route_h, route_w), (picks_h, picks)], sems
    )
    for copy in loads:
        copy.wait()
    sums = jnp.dot(picks[...], returned[...], preferred_element_type=F32)
    seqs, quarter = own.shape[0], returned.shape[1]
    for h in range(2):
        dense, first, second = (
            sums[(2 * k + h) * seqs : (2 * k + h + 1) * seqs] for k in range(3)
        )
        cols = slice(h * quarter, (h + 1) * quarter)
        total = own[:, cols].astype(F32) + (route_w[:, :1] * first + route_w[:, 1:2] * second)
        out[:, cols] = (total + weight[:, :1] * dense).astype(BF)


def local(
    tokens,
    mix_gain,
    w_query,
    w_key,
    w_value,
    w_outgate,
    w_ingate,
    w_forget,
    in_bias,
    forget_bias,
    w_mix_out,
    cell_state,
    norm_state,
    max_state,
    moe_gain,
    route_ids,
    route_weights,
    expert_gate,
    expert_up,
    expert_down,
    branch_gate,
    dense_gate,
    dense_up,
    dense_down,
):
    seqs, width = tokens.shape
    tp_count = lax.axis_size("x")
    chips = lax.axis_size("q")
    ep_count = chips * CORES
    place = lax.axis_index("x")
    cols = width // tp_count
    half = width // 2
    head_count, hd = cell_state.shape[1:3]
    pair_rows = seqs * head_count
    groups = tp_count * CORES
    share = seqs // groups
    capacity = max(2, 4 * seqs // ep_count)
    swap = [(0, 1), (1, 0)]

    right = [(i, (i + 1) % tp_count) for i in range(tp_count)]
    left = [(i, (i - 1) % tp_count) for i in range(tp_count)]
    across = [(i, (i + 2) % tp_count) for i in range(tp_count)]

    top_count = route_ids.shape[1]
    chunk_rows = 2 * (share + capacity)
    total_rows = ep_count * chunk_rows
    pack = jnp.concatenate([dense_gate.T, dense_up.T, dense_down], axis=0)
    units = dense_down.shape[0]
    front_bytes = w_query.size * 4 * 2 + cell_state.size * 4
    (
        heads, carry, written, value, new_norm, new_max, slots, select, w_mix, tok, gain,
    ) = pl.pallas_call(
        front_kernel,
        in_specs=[SMEM] + [ANY] * 16,
        out_specs=[VMEM] + [ANY] * 6 + [VMEM] * 4,
        out_shape=[
            pltpu.VMEM((seqs, head_count * hd), BF),
            pltpu.HBM((pair_rows, hd), F32),
            pltpu.HBM((pair_rows, hd), F32),
            pltpu.HBM((pair_rows, hd), F32),
            pltpu.HBM((pair_rows, hd), F32),
            pltpu.HBM((head_count, seqs), F32),
            pltpu.HBM((seqs, 128), jnp.int32),
            pltpu.VMEM((total_rows, 128), BF),
            pltpu.VMEM(w_mix_out.shape, BF),
            pltpu.VMEM(tokens.shape, BF),
            pltpu.VMEM((1, width), F32),
        ],
        scratch_shapes=[
            pltpu.VMEM((top_count, seqs), jnp.int32),
            pltpu.VMEM((seqs, 128), jnp.int32),
            pltpu.VMEM((1, width), F32),
            pltpu.VMEM((head_count, width), BF),
            pltpu.VMEM((head_count, width), BF),
            pltpu.SMEM((head_count,), F32),
            pltpu.SMEM((head_count,), F32),
            pltpu.VMEM((pair_rows, hd), F32),
            pltpu.VMEM((head_count, seqs), F32),
            pltpu.VMEM((4, *w_query.shape), BF),
            pltpu.VMEM(cell_state.shape, F32),
            pltpu.VMEM((head_count, seqs, hd), F32),
            pltpu.VMEM((pair_rows, hd), F32),
            pltpu.VMEM((pair_rows, hd), F32),
            pltpu.VMEM((pair_rows, hd), F32),
            pltpu.VMEM((pair_rows, hd), F32),
            pltpu.VMEM((head_count, seqs), F32),
            pltpu.VMEM((128, seqs * hd), BF),
            pltpu.SemaphoreType.DMA((10,)),
            pltpu.SemaphoreType.DMA((5,)),
            pltpu.SemaphoreType.DMA((6,)),
            pltpu.SemaphoreType.DMA((6,)),
        ],
        compiler_params=params(40),
        cost_estimate=pl.CostEstimate(
            flops=2 * seqs * width * 4 * head_count * hd, transcendentals=0, bytes_accessed=front_bytes
        ),
        name="front",
    )(place.reshape(1), *(far_memory(a) for a in (
        route_ids.T,
        tokens,
        mix_gain.reshape(1, width),
        w_ingate.T,
        w_forget.T,
        in_bias,
        forget_bias,
        norm_state.reshape(pair_rows, hd),
        max_state.T,
        w_query,
        w_key,
        w_value,
        w_outgate,
        cell_state,
        w_mix_out,
        moe_gain.reshape(1, width),
    )))
    heads_l = lax.ppermute(heads, "x", right)
    heads_r = lax.ppermute(heads, "x", left)
    heads_f = lax.ppermute(heads, "x", across)
    out_way = right + [(tp_count + i, tp_count + j) for i, j in left]
    back_way = left + [(tp_count + i, tp_count + j) for i, j in right]
    pack_1 = lax.ppermute(pack, ("c", "x"), out_way)
    pack_2 = lax.ppermute(pack, ("c", "x"), back_way)
    pack_3 = lax.ppermute(pack_1, ("c", "x"), out_way)
    packs = [pack, pack_1, pack_2, pack_3]
    packs += [lax.ppermute(w, "c", swap) for w in packs]

    send, own, moe_in = pl.pallas_call(
        mix_kernel,
        in_specs=[SMEM] + [VMEM] * 8,
        out_specs=[ANY, VMEM, VMEM],
        out_shape=[
            pltpu.HBM((total_rows, half), BF),
            pltpu.HBM((seqs, cols), BF),
            pltpu.HBM((seqs, width), BF),
        ],
        scratch_shapes=[pltpu.VMEM((total_rows, half), BF), pltpu.SemaphoreType.DMA((4,))],
        compiler_params=params(30),
        cost_estimate=pl.CostEstimate(
            flops=2 * seqs * width * w_mix_out.shape[0], transcendentals=0, bytes_accessed=w_mix_out.size * 2
        ),
        name="mix",
    )(
        place.reshape(1),
        *(near_memory(a) for a in (heads, heads_l, heads_r, heads_f, w_mix, tok, gain, select)),
    )
    arrived = lax.all_to_all(
        send.reshape(ep_count, chunk_rows, half), EP, split_axis=0, concat_axis=0, tiled=True
    )
    sources = ep_count * tp_count
    quarter = cols // 2
    picks, weight = pl.pallas_call(
        plan_kernel,
        in_specs=[VMEM] * 3,
        out_specs=[VMEM] * 2,
        out_shape=[
            pltpu.HBM((6 * seqs, sources * chunk_rows), BF),
            pltpu.HBM((seqs, 128), F32),
        ],
        compiler_params=params(),
        name="plan",
    )(slots, moe_in, branch_gate.reshape(1, width))
    many = ep_count * share
    back = pl.pallas_call(
        ffn_kernel,
        in_specs=[VMEM] + [ANY] * 11,
        out_specs=ANY,
        out_shape=pltpu.HBM((ep_count, tp_count, chunk_rows, quarter), BF),
        scratch_shapes=[
            pltpu.VMEM(expert_gate.shape, BF),
            pltpu.VMEM(expert_up.shape, BF),
            pltpu.VMEM(expert_down.shape, BF),
            pltpu.VMEM((8 * units, width), BF),
            pltpu.VMEM((8 * units, width), BF),
            pltpu.VMEM((8 * units, width), BF),
            pltpu.VMEM((2, many, width), BF),
            pltpu.VMEM((tp_count, ep_count, chunk_rows, quarter), BF),
            pltpu.SemaphoreType.DMA((27,)),
            pltpu.SemaphoreType.DMA((tp_count,)),
        ],
        compiler_params=params(46),
        cost_estimate=pl.CostEstimate(
            flops=6 * many * width * (8 * units + expert_down.shape[1]),
            transcendentals=0,
            bytes_accessed=6 * width * (8 * units + expert_down.shape[1]),
        ),
        name="ffn",
    )(near_memory(arrived.reshape(total_rows, half)), *(far_memory(a) for a in (
        expert_gate, expert_up, expert_down,
        *packs,
    )))
    returned = lax.all_to_all(
        back.reshape(sources, chunk_rows, quarter), ALL, split_axis=0, concat_axis=0, tiled=True
    )
    pairs = 16
    flat = pl.BlockSpec((pairs, hd), lambda i: (i, 0))
    cube = pl.BlockSpec((pairs, hd, hd), lambda i: (i, 0, 0))
    new_cell = pl.pallas_call(
        update_kernel,
        grid=(pair_rows // pairs,),
        in_specs=[flat, flat, flat, cube],
        out_specs=cube,
        out_shape=pltpu.HBM((pair_rows, hd, hd), F32),
        compiler_params=params(),
        cost_estimate=pl.CostEstimate(
            flops=3 * cell_state.size, transcendentals=0, bytes_accessed=8 * cell_state.size
        ),
        name="update",
    )(carry, written, value, far_memory(cell_state.reshape(pair_rows, hd, hd)))
    layer_out = pl.pallas_call(
        final_kernel,
        in_specs=[ANY, VMEM, ANY, ANY, ANY],
        out_specs=VMEM,
        out_shape=pltpu.HBM((seqs, cols), BF),
        scratch_shapes=[
            pltpu.VMEM((6 * seqs, sources * chunk_rows), BF),
            pltpu.VMEM((seqs, cols), BF),
            pltpu.VMEM((seqs, 128), F32),
            pltpu.VMEM(route_weights.shape, F32),
            pltpu.SemaphoreType.DMA((4,)),
        ],
        compiler_params=params(40),
        name="final",
    )(
        far_memory(picks),
        near_memory(returned.reshape(sources * chunk_rows, quarter)),
        *(far_memory(a) for a in (own, weight, route_weights)),
    )
    return (
        layer_out,
        new_cell.reshape(cell_state.shape),
        new_norm.reshape(norm_state.shape),
        new_max.T,
    )


def solution(mesh):
    ep_count, tp_count = mesh.shape["ep"], mesh.shape["tp"]
    mesh = Mesh(mesh.devices.reshape(ep_count // CORES, CORES, tp_count), ALL)
    in_specs = (
        P(EP, None),
        P(),
        P(None, "x"),
        P(None, "x"),
        P(None, "x"),
        P(None, "x"),
        P(None, "x"),
        P(None, "x"),
        P("x"),
        P("x"),
        P(),
        P(EP, "x", None, None),
        P(EP, "x", None),
        P(EP, "x"),
        P(),
        P(EP, None),
        P(EP, None),
        P(EP, None, "x"),
        P(EP, None, "x"),
        P(EP, "x", None),
        P(),
        P(None, ALL),
        P(None, ALL),
        P(ALL, None),
    )
    out_specs = (P(EP, "x"), P(EP, "x", None, None), P(EP, "x", None), P(EP, "x"))
    return jax.shard_map(local, mesh=mesh, in_specs=in_specs, out_specs=out_specs, check_vma=False)
```

```python
import jax
import jax.numpy as jnp
from jax import lax
from jax.experimental import pallas as pl
from jax.experimental.pallas import tpu as pltpu
from jax.sharding import Mesh
from jax.sharding import PartitionSpec as P


EPS = 1e-06
BF = jnp.bfloat16
F32 = jnp.float32
EP = ("q", "c")
ALL = ("q", "c", "x")
CORES = 2
VMEM = pl.BlockSpec(memory_space=pltpu.VMEM)
SMEM = pl.BlockSpec(memory_space=pltpu.SMEM)
ANY = pl.BlockSpec(memory_space=pl.ANY)


def params(mib=60):
    return pltpu.CompilerParams(vmem_limit_bytes=mib * 1024 * 1024)


def far_memory(array):
    return pltpu.with_memory_space_constraint(array, pltpu.HBM)


def near_memory(array):
    return pltpu.with_memory_space_constraint(array, pltpu.VMEM)


def nt_dot(left, right):
    return lax.dot_general(left, right, (((1,), (1,)), ((), ())), preferred_element_type=F32)


def normed_rows(rows_in, gain_vec):
    as_float = rows_in.astype(F32)
    mean = jnp.mean(as_float * as_float, axis=-1, keepdims=True)
    return (as_float * lax.rsqrt(mean + EPS) * gain_vec).astype(BF)


def log_sigmoid(x):
    return -(jnp.maximum(-x, 0.0) + jnp.log1p(jnp.exp(-jnp.abs(x))))


def gate_factors(in_pre, forget_pre, max_state):
    log_forget = log_sigmoid(forget_pre)
    new_max = jnp.maximum(log_forget + max_state, in_pre)
    return jnp.exp(log_forget + max_state - new_max), jnp.exp(in_pre - new_max), new_max


def padded_transpose(block):
    rows, cols = block.shape
    if rows < 128:
        block = jnp.concatenate([block, jnp.zeros((128 - rows, cols), block.dtype)], axis=0)
    return block.T


def start_all(pairs, sems):
    copies = [pltpu.make_async_copy(src, dst, sems.at[i]) for i, (src, dst) in enumerate(pairs)]
    for copy in copies:
        copy.start()
    return copies


def over(index, divisor):
    factor, shift = {6: (10923, 16), 24: (43691, 20)}[divisor]
    return (index * factor) >> shift


def route_tables(place, ids, select_o, slots_o):
    seqs = ids.shape[1]
    lanes = select_o.shape[1]
    row = lax.broadcasted_iota(jnp.int32, (seqs, seqs), 0)
    col = lax.broadcasted_iota(jnp.int32, (seqs, seqs), 1)
    first, second = ids[0:1], ids[1:2]
    here = lax.broadcasted_iota(jnp.int32, (seqs, lanes), 0)
    there = lax.broadcasted_iota(jnp.int32, (seqs, lanes), 1)
    slot_rows = []
    slots = jnp.zeros((seqs, lanes), jnp.int32)
    for k, own in enumerate((first, second)):
        column = jnp.sum(jnp.where(row == col, own, 0), axis=1, keepdims=True)
        same = ((column == first) | (column == second)) & (col < row)
        slot = column * 6 + jnp.sum(jnp.where(same, 1, 0), axis=1, keepdims=True)
        slots = jnp.where(there == k, slot, slots)
        slot_rows.append(
            jnp.sum(jnp.where((there & 63) == here, slot + 1, 0), axis=0, keepdims=True) - 1
        )
    slots_o[...] = slots
    line = lax.broadcasted_iota(jnp.int32, (24, lanes), 0)
    lane = lax.broadcasted_iota(jnp.int32, (24, lanes), 1)
    part = over(line, 6)
    entry = line - 6 * part
    right_side = part >> 1 == lane >> 6
    is_moe = part & 1 == 1
    wanted = jnp.where(right_side & is_moe, entry, -999)
    shared = [
        right_side & (part & 1 == 0) & ((place * CORES + c) * 6 + entry == lane & 63)
        for c in range(CORES)
    ]
    for e in range(0, select_o.shape[0] // 24, 2):
        hits = []
        for c in range(2):
            first, second = (rows - 6 * (e + c) for rows in slot_rows)
            hit = shared[c] | (wanted == first) | (wanted == second)
            hits.append(jnp.where(hit, 1.0, 0.0))
        select_o[e * 24 : (e + 2) * 24] = jnp.concatenate(hits, axis=0).astype(BF)


def front_kernel(
    place, ids_h, tok_h, gain_h, w_in_h, w_fg_h, in_bias_h, fg_bias_h, norm_h, mx_h,
    wq, wk, wv, wo, cell, w_mix_h, moe_gain_h,
    heads_o, carry_h, written_h, value_h, norm_out_h, max_h, slots_h, select_o, w_mix, tok, moe_gain,
    ids, slots, gain, w_in, w_fg, in_bias, fg_bias, norm, mx, wbuf, cbuf, num,
    carry_o, written_o, value_o, norm_o, max_o, hot, isem, wsem, csem, osem,
):
    rows, head_count, hd = cbuf.shape[:3]
    chunks = csem.shape[0]
    per = rows // chunks
    small = start_all(
        [
            (tok_h, tok), (gain_h, gain), (w_in_h, w_in), (w_fg_h, w_fg),
            (in_bias_h, in_bias), (fg_bias_h, fg_bias), (norm_h, norm), (mx_h, mx),
            (ids_h, ids), (moe_gain_h, moe_gain),
        ],
        isem,
    )
    loads = [
        pltpu.make_async_copy(w, wbuf.at[i], wsem.at[i]) for i, w in enumerate((wq, wk, wv, wo))
    ]
    parts = [
        pltpu.make_async_copy(cell.at[pl.ds(j * per, per)], cbuf.at[pl.ds(j * per, per)], csem.at[j])
        for j in range(chunks)
    ]
    later = pltpu.make_async_copy(w_mix_h, w_mix, wsem.at[4])
    for copy in (*loads[:3], *parts, loads[3], later):
        copy.start()
    small[8].wait()
    route_tables(place[0], ids, select_o, slots)
    line = lax.broadcasted_iota(jnp.int32, hot.shape, 0) & 63
    hot[...] = jnp.where(line == lax.broadcasted_iota(jnp.int32, hot.shape, 1) >> 7, 1.0, 0.0).astype(BF)
    small[0].wait()
    small[1].wait()
    normed = normed_rows(tok[...], gain[...])
    for copy in small[2:8] + small[9:]:
        copy.wait()
    loads[0].wait()
    queries = jnp.dot(normed, wbuf[0], preferred_element_type=F32)
    high = queries.astype(BF).astype(F32)
    gap = jnp.zeros((64 - rows, head_count * hd), F32)
    stacked = jnp.concatenate([high, gap, queries - high, gap], axis=0)
    turned = stacked[:, hd:].T.astype(BF)
    plain = padded_transpose(queries[:, :hd])

    def read_out(j):
        parts[j].wait()
        for b in range(j * per, (j + 1) * per, 2):
            spread = jnp.dot(turned, hot[:, b * hd : (b + 2) * hd], preferred_element_type=F32)
            for k in range(2):
                num[1, b + k : b + k + 1] = jnp.sum(
                    spread[:, k * hd : (k + 1) * hd] * cbuf[b + k, 1], axis=0, keepdims=True
                )
                num[0, b + k : b + k + 1] = jnp.sum(
                    plain[:, b + k : b + k + 1] * cbuf[b + k, 0], axis=0, keepdims=True
                )

    in_row = nt_dot(w_in[...], normed)
    fg_row = nt_dot(w_fg[...], normed)
    factors = []
    for h in range(head_count):
        found = gate_factors(
            in_row[h : h + 1] + in_bias[h], fg_row[h : h + 1] + fg_bias[h], mx[h : h + 1]
        )
        max_o[h : h + 1] = found[2]
        factors += found
    factors.append(jnp.zeros((8 - len(factors), rows), F32))
    same = lax.broadcasted_iota(jnp.int32, (rows, rows), 0) == lax.broadcasted_iota(
        jnp.int32, (rows, rows), 1
    )
    columns = lax.dot_general(
        same.astype(F32),
        jnp.concatenate(factors, axis=0),
        (((1,), (1,)), ((), ())),
        preferred_element_type=F32,
        precision=lax.Precision.HIGHEST,
    )

    def project(i):
        loads[i].wait()
        return jnp.dot(normed, wbuf[i], preferred_element_type=F32)

    keys = project(1) * hd ** (-0.5)
    values = project(2)
    kept = []
    for h in range(head_count):
        cols = slice(h * hd, (h + 1) * hd)
        carry, write, new_max = (columns[:, 3 * h + k : 3 * h + k + 1] for k in range(3))
        query, value = queries[:, cols], values[:, cols]
        written = write * keys[:, cols]
        at = pl.ds(h, rows, stride=head_count)
        new_norm = carry * norm[at, :] + written
        norm_o[at, :] = new_norm
        written_o[at, :] = written
        value_o[at, :] = value
        carry_o[at, :] = jnp.broadcast_to(carry, (rows, hd))
        denominator = jnp.sum(query * new_norm, axis=-1, keepdims=True)
        floor = jnp.maximum(jnp.abs(denominator), jnp.exp(-new_max))
        added = jnp.sum(query * written, axis=-1, keepdims=True) * value
        kept.append((carry, added, floor))
    stores = start_all(
        [
            (carry_o, carry_h), (written_o, written_h), (value_o, value_h),
            (norm_o, norm_out_h), (max_o, max_h), (slots, slots_h),
        ],
        osem,
    )
    for j in range(chunks):
        read_out(j)
    opened = jax.nn.sigmoid(project(3))
    for h in range(head_count):
        cols = slice(h * hd, (h + 1) * hd)
        carry, added, floor = kept[h]
        heads_o[:, cols] = (opened[:, cols] * ((carry * num[h] + added) / floor)).astype(BF)
    for copy in stores:
        copy.wait()
    later.wait()


def update_kernel(carry, written, value, cell, out):
    turned = padded_transpose(written[...])
    for p in range(cell.shape[0]):
        out[p] = carry[p : p + 1] * cell[p] + turned[:, p : p + 1] * value[p : p + 1]


def plan_kernel(slots, moe_in, branch, picks_o, weight_o):
    logit = jnp.sum(moe_in[...].astype(F32) * branch[...].astype(F32), axis=-1, keepdims=True)
    weight_o[...] = jnp.broadcast_to(jax.nn.sigmoid(logit), weight_o.shape)
    seqs = slots.shape[0]
    lanes = picks_o.shape[1]
    lane = lax.broadcasted_iota(jnp.int32, (1, lanes), 1)
    source = over(lane, 24)
    inner = lane - 24 * source
    part = over(inner, 6)
    entry = inner - 6 * part
    side, is_moe = part >> 1, part & 1
    from_x, from_c, from_e = source & 3, (source >> 2) & 1, source >> 2
    dense_row = jnp.where(is_moe == 0, (from_x * CORES + from_c) * 6 + entry, -1)
    slot = jnp.where(is_moe == 1, from_e * 6 + entry, -1)
    row = lax.broadcasted_iota(jnp.int32, (seqs, 1), 0)
    for k in range(3):
        if k == 0:
            hit = jnp.where(dense_row == row, 1.0, 0.0)
        else:
            hit = jnp.where(slot == slots[:, k - 1 : k], 1.0, 0.0)
        for h in range(2):
            at = (2 * k + h) * seqs
            picks_o[at : at + seqs] = jnp.where(side == h, hit, 0.0).astype(BF)


def mix_kernel(
    place, heads, heads_l, heads_r, heads_f, w_mix, tok, gain, select,
    send_h, own_o, moe_o,
    send, sems,
):
    width = heads.shape[1]
    mixed_proj = None
    for turn, block in ((0, heads), (3, heads_l), (1, heads_r), (2, heads_f)):
        start = pl.multiple_of(((place[0] + turn) & 3) * width, width)
        part = jnp.dot(block[...], w_mix[pl.ds(start, width)], preferred_element_type=F32)
        mixed_proj = part if mixed_proj is None else mixed_proj + part
    residual = (tok[...].astype(F32) + mixed_proj).astype(BF)
    moe_in = normed_rows(residual, gain[...])
    half = send.shape[1]
    gap = jnp.zeros((select.shape[1] // 2 - moe_in.shape[0], half), BF)
    stacked = jnp.concatenate([moe_in[:, :half], gap, moe_in[:, half:], gap], axis=0)
    chunks = sems.shape[0]
    lines = send.shape[0] // chunks
    stores = []
    for j in range(chunks):
        at = pl.ds(j * lines, lines)
        send[at] = jnp.dot(select[at], stacked, preferred_element_type=F32).astype(BF)
        stores.append(pltpu.make_async_copy(send.at[at], send_h.at[at], sems.at[j]))
        stores[j].start()
    moe_o[...] = moe_in
    cols = own_o.shape[1]
    own = residual[:, :cols]
    for k in range(1, residual.shape[1] // cols):
        own = jnp.where(place[0] == k, residual[:, k * cols : (k + 1) * cols], own)
    own_o[...] = own
    for copy in stores:
        copy.wait()


def grouped_row(index, lines):
    source = over(index, 24)
    inner = index - 24 * source
    part = over(inner, 6)
    return part * lines + source * 6 + inner - 6 * part


def ffn_kernel(abuf, e_gate, e_up, e_down, *rest):
    packs, rest = rest[:8], rest[8:]
    out, egbuf, eubuf, edbuf, gbuf, ubuf, dbuf, xbuf, obuf, sems, osems = rest
    units = packs[0].shape[0] // 3
    pairs = []
    for b, pack in enumerate(packs):
        rows = pl.ds(b * units, units)
        pairs.append((pack.at[pl.ds(0, units)], gbuf.at[rows]))
        pairs.append((pack.at[pl.ds(units, units)], ubuf.at[rows]))
        pairs.append((pack.at[pl.ds(2 * units, units)], dbuf.at[rows]))
    pairs += [(e_gate, egbuf), (e_up, eubuf), (e_down, edbuf)]
    loads = start_all(pairs, sems)
    size, half = abuf.shape
    block = 192
    groups = size // block
    lines = block // 4
    row = lax.broadcasted_iota(jnp.int32, (block, 1), 0)
    col = lax.broadcasted_iota(jnp.int32, (1, block), 1)
    gather = jnp.where(grouped_row(col, lines) == row, 1.0, 0.0).astype(BF)
    spread = jnp.where(grouped_row(row, lines) == col, 1.0, 0.0).astype(BF)
    for g in range(groups):
        sorted_rows = jnp.dot(
            gather, abuf[g * block : (g + 1) * block], preferred_element_type=F32
        ).astype(BF)
        for part in range(4):
            xbuf[
                part % 2,
                g * lines : (g + 1) * lines,
                (part // 2) * half : (part // 2 + 1) * half,
            ] = sorted_rows[part * lines : (part + 1) * lines]
    tok = xbuf[0]
    total = None
    for side in range(2):
        for copy in loads[12 * side : 12 + 12 * side]:
            copy.wait()
        rows = slice(side * 4 * units, (side + 1) * 4 * units)
        hidden = (jax.nn.silu(nt_dot(tok, gbuf[rows])) * nt_dot(tok, ubuf[rows])).astype(BF)
        part = jnp.dot(hidden, dbuf[rows], preferred_element_type=F32)
        total = part if total is None else total + part
    total = total.astype(BF)
    tok = xbuf[1]
    loads[24].wait()
    loads[25].wait()
    gate_proj = jnp.dot(tok, egbuf[0], preferred_element_type=F32)
    up_proj = jnp.dot(tok, eubuf[0], preferred_element_type=F32)
    hidden = (jax.nn.silu(gate_proj) * up_proj).astype(BF)
    loads[26].wait()
    expert_out = jnp.dot(hidden, edbuf[0], preferred_element_type=F32).astype(BF)
    peers, quarter = obuf.shape[0], obuf.shape[3]
    held = obuf.shape[1] // groups
    stores = []
    for s in range(peers):
        for g in range(groups):
            rows = slice(g * lines, (g + 1) * lines)
            sides = []
            for h in range(2):
                at = (2 * s + h) * quarter
                sides += [total[rows, at : at + quarter], expert_out[rows, at : at + quarter]]
            mixed = jnp.dot(spread, jnp.concatenate(sides, axis=0), preferred_element_type=F32)
            obuf[s, g * held : (g + 1) * held] = mixed.reshape(held, -1, quarter).astype(BF)
        stores.append(pltpu.make_async_copy(obuf.at[s], out.at[:, s], osems.at[s]))
        stores[s].start()
    for copy in stores:
        copy.wait()


def final_kernel(
    picks_h, returned, own_h, weight_h, route_h, out, picks, own, weight, route_w, sems
):
    lanes = picks.shape[1] // 3
    thirds = [pl.ds(k * lanes, lanes) for k in range(3)]
    loads = start_all(
        [(picks_h.at[:, at], picks.at[:, at]) for at in thirds]
        + [(own_h, own), (weight_h, weight), (route_h, route_w)],
        sems,
    )
    sums = None
    for k, at in enumerate(thirds):
        loads[k].wait()
        part = jnp.dot(picks[:, at], returned[at], preferred_element_type=F32)
        sums = part if sums is None else sums + part
    for copy in loads[3:]:
        copy.wait()
    seqs, quarter = own.shape[0], returned.shape[1]
    for h in range(2):
        dense, first, second = (
            sums[(2 * k + h) * seqs : (2 * k + h + 1) * seqs] for k in range(3)
        )
        cols = slice(h * quarter, (h + 1) * quarter)
        total = own[:, cols].astype(F32) + (route_w[:, :1] * first + route_w[:, 1:2] * second)
        out[:, cols] = (total + weight[:, :1] * dense).astype(BF)


def local(
    tokens,
    mix_gain,
    w_query,
    w_key,
    w_value,
    w_outgate,
    w_ingate,
    w_forget,
    in_bias,
    forget_bias,
    w_mix_out,
    cell_state,
    norm_state,
    max_state,
    moe_gain,
    route_ids,
    route_weights,
    expert_gate,
    expert_up,
    expert_down,
    branch_gate,
    dense_gate,
    dense_up,
    dense_down,
):
    seqs, width = tokens.shape
    tp_count = lax.axis_size("x")
    chips = lax.axis_size("q")
    ep_count = chips * CORES
    place = lax.axis_index("x")
    cols = width // tp_count
    half = width // 2
    head_count, hd = cell_state.shape[1:3]
    pair_rows = seqs * head_count
    groups = tp_count * CORES
    share = seqs // groups
    capacity = max(2, 4 * seqs // ep_count)
    swap = [(0, 1), (1, 0)]

    right = [(i, (i + 1) % tp_count) for i in range(tp_count)]
    left = [(i, (i - 1) % tp_count) for i in range(tp_count)]
    across = [(i, (i + 2) % tp_count) for i in range(tp_count)]

    top_count = route_ids.shape[1]
    chunk_rows = 2 * (share + capacity)
    total_rows = ep_count * chunk_rows
    pack = jnp.concatenate([dense_gate.T, dense_up.T, dense_down], axis=0)
    units = dense_down.shape[0]
    front_bytes = w_query.size * 4 * 2 + cell_state.size * 4
    (
        heads, carry, written, value, new_norm, new_max, slots, select, w_mix, tok, gain,
    ) = pl.pallas_call(
        front_kernel,
        in_specs=[SMEM] + [ANY] * 16,
        out_specs=[VMEM] + [ANY] * 6 + [VMEM] * 4,
        out_shape=[
            pltpu.VMEM((seqs, head_count * hd), BF),
            pltpu.HBM((pair_rows, hd), F32),
            pltpu.HBM((pair_rows, hd), F32),
            pltpu.HBM((pair_rows, hd), F32),
            pltpu.HBM((pair_rows, hd), F32),
            pltpu.HBM((head_count, seqs), F32),
            pltpu.HBM((seqs, 128), jnp.int32),
            pltpu.VMEM((total_rows, 128), BF),
            pltpu.VMEM(w_mix_out.shape, BF),
            pltpu.VMEM(tokens.shape, BF),
            pltpu.VMEM((1, width), F32),
        ],
        scratch_shapes=[
            pltpu.VMEM((top_count, seqs), jnp.int32),
            pltpu.VMEM((seqs, 128), jnp.int32),
            pltpu.VMEM((1, width), F32),
            pltpu.VMEM((head_count, width), BF),
            pltpu.VMEM((head_count, width), BF),
            pltpu.SMEM((head_count,), F32),
            pltpu.SMEM((head_count,), F32),
            pltpu.VMEM((pair_rows, hd), F32),
            pltpu.VMEM((head_count, seqs), F32),
            pltpu.VMEM((4, *w_query.shape), BF),
            pltpu.VMEM(cell_state.shape, F32),
            pltpu.VMEM((head_count, seqs, hd), F32),
            pltpu.VMEM((pair_rows, hd), F32),
            pltpu.VMEM((pair_rows, hd), F32),
            pltpu.VMEM((pair_rows, hd), F32),
            pltpu.VMEM((pair_rows, hd), F32),
            pltpu.VMEM((head_count, seqs), F32),
            pltpu.VMEM((128, seqs * hd), BF),
            pltpu.SemaphoreType.DMA((10,)),
            pltpu.SemaphoreType.DMA((5,)),
            pltpu.SemaphoreType.DMA((6,)),
            pltpu.SemaphoreType.DMA((6,)),
        ],
        compiler_params=params(40),
        cost_estimate=pl.CostEstimate(
            flops=2 * seqs * width * 4 * head_count * hd, transcendentals=0, bytes_accessed=front_bytes
        ),
        name="front",
    )(place.reshape(1), *(far_memory(a) for a in (
        route_ids.T,
        tokens,
        mix_gain.reshape(1, width),
        w_ingate.T,
        w_forget.T,
        in_bias,
        forget_bias,
        norm_state.reshape(pair_rows, hd),
        max_state.T,
        w_query,
        w_key,
        w_value,
        w_outgate,
        cell_state,
        w_mix_out,
        moe_gain.reshape(1, width),
    )))
    heads_l = lax.ppermute(heads, "x", right)
    heads_r = lax.ppermute(heads, "x", left)
    heads_f = lax.ppermute(heads, "x", across)
    out_way = right + [(tp_count + i, tp_count + j) for i, j in left]
    back_way = left + [(tp_count + i, tp_count + j) for i, j in right]
    pack_1 = lax.ppermute(pack, ("c", "x"), out_way)
    pack_2 = lax.ppermute(pack, ("c", "x"), back_way)
    pack_3 = lax.ppermute(pack_1, ("c", "x"), out_way)
    packs = [pack, pack_1, pack_2, pack_3]
    packs += [lax.ppermute(w, "c", swap) for w in packs]

    send, own, moe_in = pl.pallas_call(
        mix_kernel,
        in_specs=[SMEM] + [VMEM] * 8,
        out_specs=[ANY, VMEM, VMEM],
        out_shape=[
            pltpu.HBM((total_rows, half), BF),
            pltpu.HBM((seqs, cols), BF),
            pltpu.HBM((seqs, width), BF),
        ],
        scratch_shapes=[pltpu.VMEM((total_rows, half), BF), pltpu.SemaphoreType.DMA((4,))],
        compiler_params=params(30),
        cost_estimate=pl.CostEstimate(
            flops=2 * seqs * width * w_mix_out.shape[0], transcendentals=0, bytes_accessed=w_mix_out.size * 2
        ),
        name="mix",
    )(
        place.reshape(1),
        *(near_memory(a) for a in (heads, heads_l, heads_r, heads_f, w_mix, tok, gain, select)),
    )
    arrived = lax.all_to_all(
        send.reshape(ep_count, chunk_rows, half), EP, split_axis=0, concat_axis=0, tiled=True
    )
    sources = ep_count * tp_count
    quarter = cols // 2
    picks, weight = pl.pallas_call(
        plan_kernel,
        in_specs=[VMEM] * 3,
        out_specs=[VMEM] * 2,
        out_shape=[
            pltpu.HBM((6 * seqs, sources * chunk_rows), BF),
            pltpu.HBM((seqs, 128), F32),
        ],
        compiler_params=params(),
        name="plan",
    )(slots, moe_in, branch_gate.reshape(1, width))
    many = ep_count * share
    back = pl.pallas_call(
        ffn_kernel,
        in_specs=[VMEM] + [ANY] * 11,
        out_specs=ANY,
        out_shape=pltpu.HBM((ep_count, tp_count, chunk_rows, quarter), BF),
        scratch_shapes=[
            pltpu.VMEM(expert_gate.shape, BF),
            pltpu.VMEM(expert_up.shape, BF),
            pltpu.VMEM(expert_down.shape, BF),
            pltpu.VMEM((8 * units, width), BF),
            pltpu.VMEM((8 * units, width), BF),
            pltpu.VMEM((8 * units, width), BF),
            pltpu.VMEM((2, many, width), BF),
            pltpu.VMEM((tp_count, ep_count, chunk_rows, quarter), BF),
            pltpu.SemaphoreType.DMA((27,)),
            pltpu.SemaphoreType.DMA((tp_count,)),
        ],
        compiler_params=params(46),
        cost_estimate=pl.CostEstimate(
            flops=6 * many * width * (8 * units + expert_down.shape[1]),
            transcendentals=0,
            bytes_accessed=6 * width * (8 * units + expert_down.shape[1]),
        ),
        name="ffn",
    )(near_memory(arrived.reshape(total_rows, half)), *(far_memory(a) for a in (
        expert_gate, expert_up, expert_down,
        *packs,
    )))
    returned = lax.all_to_all(
        back.reshape(sources, chunk_rows, quarter), ALL, split_axis=0, concat_axis=0, tiled=True
    )
    pairs = 16
    flat = pl.BlockSpec((pairs, hd), lambda i: (i, 0))
    cube = pl.BlockSpec((pairs, hd, hd), lambda i: (i, 0, 0))
    new_cell = pl.pallas_call(
        update_kernel,
        grid=(pair_rows // pairs,),
        in_specs=[flat, flat, flat, cube],
        out_specs=cube,
        out_shape=pltpu.HBM((pair_rows, hd, hd), F32),
        compiler_params=params(),
        cost_estimate=pl.CostEstimate(
            flops=3 * cell_state.size, transcendentals=0, bytes_accessed=8 * cell_state.size
        ),
        name="update",
    )(carry, written, value, far_memory(cell_state.reshape(pair_rows, hd, hd)))
    layer_out = pl.pallas_call(
        final_kernel,
        in_specs=[ANY, VMEM, ANY, ANY, ANY],
        out_specs=VMEM,
        out_shape=pltpu.HBM((seqs, cols), BF),
        scratch_shapes=[
            pltpu.VMEM((6 * seqs, sources * chunk_rows), BF),
            pltpu.VMEM((seqs, cols), BF),
            pltpu.VMEM((seqs, 128), F32),
            pltpu.VMEM(route_weights.shape, F32),
            pltpu.SemaphoreType.DMA((6,)),
        ],
        compiler_params=params(40),
        name="final",
    )(
        far_memory(picks),
        near_memory(returned.reshape(sources * chunk_rows, quarter)),
        *(far_memory(a) for a in (own, weight, route_weights)),
    )
    return (
        layer_out,
        new_cell.reshape(cell_state.shape),
        new_norm.reshape(norm_state.shape),
        new_max.T,
    )


def solution(mesh):
    ep_count, tp_count = mesh.shape["ep"], mesh.shape["tp"]
    mesh = Mesh(mesh.devices.reshape(ep_count // CORES, CORES, tp_count), ALL)
    in_specs = (
        P(EP, None),
        P(),
        P(None, "x"),
        P(None, "x"),
        P(None, "x"),
        P(None, "x"),
        P(None, "x"),
        P(None, "x"),
        P("x"),
        P("x"),
        P(),
        P(EP, "x", None, None),
        P(EP, "x", None),
        P(EP, "x"),
        P(),
        P(EP, None),
        P(EP, None),
        P(EP, None, "x"),
        P(EP, None, "x"),
        P(EP, "x", None),
        P(),
        P(None, ALL),
        P(None, ALL),
        P(ALL, None),
    )
    out_specs = (P(EP, "x"), P(EP, "x", None, None), P(EP, "x", None), P(EP, "x"))
    return jax.shard_map(local, mesh=mesh, in_specs=in_specs, out_specs=out_specs, check_vma=False)
```

```python
import jax
import jax.numpy as jnp
from jax import lax
from jax.experimental import pallas as pl
from jax.experimental.pallas import tpu as pltpu
from jax.sharding import Mesh
from jax.sharding import PartitionSpec as P


EPS = 1e-06
BF = jnp.bfloat16
F32 = jnp.float32
EP = ("q", "c")
ALL = ("q", "c", "x")
CORES = 2
VMEM = pl.BlockSpec(memory_space=pltpu.VMEM)
SMEM = pl.BlockSpec(memory_space=pltpu.SMEM)
ANY = pl.BlockSpec(memory_space=pl.ANY)


def params(mib=60):
    return pltpu.CompilerParams(vmem_limit_bytes=mib * 1024 * 1024)


def far_memory(array):
    return pltpu.with_memory_space_constraint(array, pltpu.HBM)


def near_memory(array):
    return pltpu.with_memory_space_constraint(array, pltpu.VMEM)


def nt_dot(left, right):
    return lax.dot_general(left, right, (((1,), (1,)), ((), ())), preferred_element_type=F32)


def normed_rows(rows_in, gain_vec):
    as_float = rows_in.astype(F32)
    mean = jnp.mean(as_float * as_float, axis=-1, keepdims=True)
    return (as_float * lax.rsqrt(mean + EPS) * gain_vec).astype(BF)


def log_sigmoid(x):
    return -(jnp.maximum(-x, 0.0) + jnp.log1p(jnp.exp(-jnp.abs(x))))


def gate_factors(in_pre, forget_pre, max_state):
    log_forget = log_sigmoid(forget_pre)
    new_max = jnp.maximum(log_forget + max_state, in_pre)
    return jnp.exp(log_forget + max_state - new_max), jnp.exp(in_pre - new_max), new_max


def padded_transpose(block):
    rows, cols = block.shape
    if rows < 128:
        block = jnp.concatenate([block, jnp.zeros((128 - rows, cols), block.dtype)], axis=0)
    return block.T


def start_all(pairs, sems):
    copies = [pltpu.make_async_copy(src, dst, sems.at[i]) for i, (src, dst) in enumerate(pairs)]
    for copy in copies:
        copy.start()
    return copies


def over(index, divisor):
    factor, shift = {6: (10923, 16), 24: (43691, 20)}[divisor]
    return (index * factor) >> shift


def route_tables(place, ids, select_o, slots_o):
    seqs = ids.shape[1]
    lanes = select_o.shape[1]
    row = lax.broadcasted_iota(jnp.int32, (seqs, seqs), 0)
    col = lax.broadcasted_iota(jnp.int32, (seqs, seqs), 1)
    first, second = ids[0:1], ids[1:2]
    here = lax.broadcasted_iota(jnp.int32, (seqs, lanes), 0)
    there = lax.broadcasted_iota(jnp.int32, (seqs, lanes), 1)
    slot_rows = []
    slots = jnp.zeros((seqs, lanes), jnp.int32)
    for k, own in enumerate((first, second)):
        column = jnp.sum(jnp.where(row == col, own, 0), axis=1, keepdims=True)
        same = ((column == first) | (column == second)) & (col < row)
        slot = column * 6 + jnp.sum(jnp.where(same, 1, 0), axis=1, keepdims=True)
        slots = jnp.where(there == k, slot, slots)
        slot_rows.append(
            jnp.sum(jnp.where((there & 63) == here, slot + 1, 0), axis=0, keepdims=True) - 1
        )
    slots_o[...] = slots
    line = lax.broadcasted_iota(jnp.int32, (24, lanes), 0)
    lane = lax.broadcasted_iota(jnp.int32, (24, lanes), 1)
    part = over(line, 6)
    entry = line - 6 * part
    right_side = part >> 1 == lane >> 6
    is_moe = part & 1 == 1
    wanted = jnp.where(right_side & is_moe, entry, -999)
    shared = [
        right_side & (part & 1 == 0) & ((place * CORES + c) * 6 + entry == lane & 63)
        for c in range(CORES)
    ]
    for e in range(0, select_o.shape[0] // 24, 2):
        hits = []
        for c in range(2):
            first, second = (rows - 6 * (e + c) for rows in slot_rows)
            hit = shared[c] | (wanted == first) | (wanted == second)
            hits.append(jnp.where(hit, 1.0, 0.0))
        select_o[e * 24 : (e + 2) * 24] = jnp.concatenate(hits, axis=0).astype(BF)


def front_kernel(
    place, ids_h, tok_h, gain_h, w_in_h, w_fg_h, in_bias_h, fg_bias_h, norm_h, mx_h,
    wq, wk, wv, wo, cell, w_mix_h, moe_gain_h,
    heads_o, carry_h, written_h, value_h, norm_out_h, max_h, slots_h, select_o, w_mix, tok, moe_gain,
    ids, slots, gain, w_in, w_fg, in_bias, fg_bias, norm, mx, wbuf, cbuf, num,
    carry_o, written_o, value_o, norm_o, max_o, hot, isem, wsem, csem, osem,
):
    rows, head_count, hd = cbuf.shape[:3]
    chunks = csem.shape[0]
    per = rows // chunks
    small = start_all(
        [
            (tok_h, tok), (gain_h, gain), (w_in_h, w_in), (w_fg_h, w_fg),
            (in_bias_h, in_bias), (fg_bias_h, fg_bias), (norm_h, norm), (mx_h, mx),
            (ids_h, ids), (moe_gain_h, moe_gain),
        ],
        isem,
    )
    loads = [
        pltpu.make_async_copy(w, wbuf.at[i], wsem.at[i]) for i, w in enumerate((wq, wk, wv, wo))
    ]
    parts = [
        pltpu.make_async_copy(cell.at[pl.ds(j * per, per)], cbuf.at[pl.ds(j * per, per)], csem.at[j])
        for j in range(chunks)
    ]
    later = pltpu.make_async_copy(w_mix_h, w_mix, wsem.at[4])
    for copy in (*loads[:3], *parts, loads[3], later):
        copy.start()
    small[8].wait()
    route_tables(place[0], ids, select_o, slots)
    line = lax.broadcasted_iota(jnp.int32, hot.shape, 0) & 63
    hot[...] = jnp.where(line == lax.broadcasted_iota(jnp.int32, hot.shape, 1) >> 7, 1.0, 0.0).astype(BF)
    small[0].wait()
    small[1].wait()
    normed = normed_rows(tok[...], gain[...])
    for copy in small[2:8] + small[9:]:
        copy.wait()
    loads[0].wait()
    queries = jnp.dot(normed, wbuf[0], preferred_element_type=F32)
    high = queries.astype(BF).astype(F32)
    gap = jnp.zeros((64 - rows, head_count * hd), F32)
    stacked = jnp.concatenate([high, gap, queries - high, gap], axis=0)
    turned = stacked[:, hd:].T.astype(BF)
    plain = padded_transpose(queries[:, :hd])

    def read_out(j):
        parts[j].wait()
        for b in range(j * per, (j + 1) * per, 2):
            spread = jnp.dot(turned, hot[:, b * hd : (b + 2) * hd], preferred_element_type=F32)
            for k in range(2):
                num[1, b + k : b + k + 1] = jnp.sum(
                    spread[:, k * hd : (k + 1) * hd] * cbuf[b + k, 1], axis=0, keepdims=True
                )
                num[0, b + k : b + k + 1] = jnp.sum(
                    plain[:, b + k : b + k + 1] * cbuf[b + k, 0], axis=0, keepdims=True
                )

    in_row = nt_dot(w_in[...], normed)
    fg_row = nt_dot(w_fg[...], normed)
    factors = []
    for h in range(head_count):
        found = gate_factors(
            in_row[h : h + 1] + in_bias[h], fg_row[h : h + 1] + fg_bias[h], mx[h : h + 1]
        )
        max_o[h : h + 1] = found[2]
        factors += found
    factors.append(jnp.zeros((8 - len(factors), rows), F32))
    same = lax.broadcasted_iota(jnp.int32, (rows, rows), 0) == lax.broadcasted_iota(
        jnp.int32, (rows, rows), 1
    )
    columns = lax.dot_general(
        same.astype(F32),
        jnp.concatenate(factors, axis=0),
        (((1,), (1,)), ((), ())),
        preferred_element_type=F32,
        precision=lax.Precision.HIGHEST,
    )

    def project(i):
        loads[i].wait()
        return jnp.dot(normed, wbuf[i], preferred_element_type=F32)

    keys = project(1) * hd ** (-0.5)
    values = project(2)
    kept = []
    for h in range(head_count):
        cols = slice(h * hd, (h + 1) * hd)
        carry, write, new_max = (columns[:, 3 * h + k : 3 * h + k + 1] for k in range(3))
        query, value = queries[:, cols], values[:, cols]
        written = write * keys[:, cols]
        at = pl.ds(h, rows, stride=head_count)
        new_norm = carry * norm[at, :] + written
        norm_o[at, :] = new_norm
        written_o[at, :] = written
        value_o[at, :] = value
        carry_o[at, :] = jnp.broadcast_to(carry, (rows, hd))
        denominator = jnp.sum(query * new_norm, axis=-1, keepdims=True)
        floor = jnp.maximum(jnp.abs(denominator), jnp.exp(-new_max))
        added = jnp.sum(query * written, axis=-1, keepdims=True) * value
        kept.append((carry, added, floor))
    stores = start_all(
        [
            (carry_o, carry_h), (written_o, written_h), (value_o, value_h),
            (norm_o, norm_out_h), (max_o, max_h), (slots, slots_h),
        ],
        osem,
    )
    for j in range(chunks):
        read_out(j)
    opened = jax.nn.sigmoid(project(3))
    for h in range(head_count):
        cols = slice(h * hd, (h + 1) * hd)
        carry, added, floor = kept[h]
        heads_o[:, cols] = (opened[:, cols] * ((carry * num[h] + added) / floor)).astype(BF)
    for copy in stores:
        copy.wait()
    later.wait()


def update_kernel(carry, written, value, cell, out):
    turned = padded_transpose(written[...])
    for p in range(cell.shape[0]):
        out[p] = carry[p : p + 1] * cell[p] + turned[:, p : p + 1] * value[p : p + 1]


def plan_kernel(slots, moe_in, branch, picks_o, weight_o):
    logit = jnp.sum(moe_in[...].astype(F32) * branch[...].astype(F32), axis=-1, keepdims=True)
    weight_o[...] = jnp.broadcast_to(jax.nn.sigmoid(logit), weight_o.shape)
    seqs = slots.shape[0]
    lanes = picks_o.shape[1]
    lane = lax.broadcasted_iota(jnp.int32, (1, lanes), 1)
    source = over(lane, 24)
    inner = lane - 24 * source
    part = over(inner, 6)
    entry = inner - 6 * part
    side, is_moe = part >> 1, part & 1
    from_x, from_c, from_e = source & 3, (source >> 2) & 1, source >> 2
    dense_row = jnp.where(is_moe == 0, (from_x * CORES + from_c) * 6 + entry, -1)
    slot = jnp.where(is_moe == 1, from_e * 6 + entry, -1)
    row = lax.broadcasted_iota(jnp.int32, (seqs, 1), 0)
    for k in range(3):
        if k == 0:
            hit = jnp.where(dense_row == row, 1.0, 0.0)
        else:
            hit = jnp.where(slot == slots[:, k - 1 : k], 1.0, 0.0)
        for h in range(2):
            at = (2 * k + h) * seqs
            picks_o[at : at + seqs] = jnp.where(side == h, hit, 0.0).astype(BF)


def mix_kernel(
    place, heads, heads_l, heads_r, heads_f, w_mix, tok, gain, select,
    send_h, own_h, moe_h,
    send, own_o, moe_o, sems,
):
    width = heads.shape[1]
    mixed_proj = None
    for turn, block in ((0, heads), (3, heads_l), (1, heads_r), (2, heads_f)):
        start = pl.multiple_of(((place[0] + turn) & 3) * width, width)
        part = jnp.dot(block[...], w_mix[pl.ds(start, width)], preferred_element_type=F32)
        mixed_proj = part if mixed_proj is None else mixed_proj + part
    residual = (tok[...].astype(F32) + mixed_proj).astype(BF)
    moe_in = normed_rows(residual, gain[...])
    half = send.shape[1]
    gap = jnp.zeros((select.shape[1] // 2 - moe_in.shape[0], half), BF)
    stacked = jnp.concatenate([moe_in[:, :half], gap, moe_in[:, half:], gap], axis=0)
    moe_o[...] = moe_in
    cols = own_o.shape[1]
    own = residual[:, :cols]
    for k in range(1, residual.shape[1] // cols):
        own = jnp.where(place[0] == k, residual[:, k * cols : (k + 1) * cols], own)
    own_o[...] = own
    chunks = sems.shape[0] - 2
    lines = send.shape[0] // chunks
    stores = [
        pltpu.make_async_copy(own_o, own_h, sems.at[chunks]),
        pltpu.make_async_copy(moe_o, moe_h, sems.at[chunks + 1]),
    ]
    for copy in stores:
        copy.start()
    for j in range(chunks):
        at = pl.ds(j * lines, lines)
        send[at] = jnp.dot(select[at], stacked, preferred_element_type=F32).astype(BF)
        stores.append(pltpu.make_async_copy(send.at[at], send_h.at[at], sems.at[j]))
        stores[-1].start()
    for copy in stores:
        copy.wait()


def grouped_row(index, lines):
    source = over(index, 24)
    inner = index - 24 * source
    part = over(inner, 6)
    return part * lines + source * 6 + inner - 6 * part


def ffn_kernel(abuf, e_gate, e_up, e_down, *rest):
    packs, rest = rest[:8], rest[8:]
    out, egbuf, eubuf, edbuf, gbuf, ubuf, dbuf, xbuf, obuf, sems, osems = rest
    units = packs[0].shape[0] // 3
    pairs = []
    for b, pack in enumerate(packs):
        rows = pl.ds(b * units, units)
        pairs.append((pack.at[pl.ds(0, units)], gbuf.at[rows]))
        pairs.append((pack.at[pl.ds(units, units)], ubuf.at[rows]))
        pairs.append((pack.at[pl.ds(2 * units, units)], dbuf.at[rows]))
    pairs += [(e_gate, egbuf), (e_up, eubuf), (e_down, edbuf)]
    loads = start_all(pairs, sems)
    size, half = abuf.shape
    block = 192
    groups = size // block
    lines = block // 4
    row = lax.broadcasted_iota(jnp.int32, (block, 1), 0)
    col = lax.broadcasted_iota(jnp.int32, (1, block), 1)
    gather = jnp.where(grouped_row(col, lines) == row, 1.0, 0.0).astype(BF)
    spread = jnp.where(grouped_row(row, lines) == col, 1.0, 0.0).astype(BF)
    for g in range(groups):
        sorted_rows = jnp.dot(
            gather, abuf[g * block : (g + 1) * block], preferred_element_type=F32
        ).astype(BF)
        for part in range(4):
            xbuf[
                part % 2,
                g * lines : (g + 1) * lines,
                (part // 2) * half : (part // 2 + 1) * half,
            ] = sorted_rows[part * lines : (part + 1) * lines]
    tok = xbuf[0]
    total = None
    for side in range(2):
        for copy in loads[12 * side : 12 + 12 * side]:
            copy.wait()
        rows = slice(side * 4 * units, (side + 1) * 4 * units)
        hidden = (jax.nn.silu(nt_dot(tok, gbuf[rows])) * nt_dot(tok, ubuf[rows])).astype(BF)
        part = jnp.dot(hidden, dbuf[rows], preferred_element_type=F32)
        total = part if total is None else total + part
    total = total.astype(BF)
    tok = xbuf[1]
    loads[24].wait()
    loads[25].wait()
    gate_proj = jnp.dot(tok, egbuf[0], preferred_element_type=F32)
    up_proj = jnp.dot(tok, eubuf[0], preferred_element_type=F32)
    hidden = (jax.nn.silu(gate_proj) * up_proj).astype(BF)
    loads[26].wait()
    expert_out = jnp.dot(hidden, edbuf[0], preferred_element_type=F32).astype(BF)
    peers, quarter = obuf.shape[0], obuf.shape[3]
    held = obuf.shape[1] // groups
    stores = []
    for s in range(peers):
        for g in range(groups):
            rows = slice(g * lines, (g + 1) * lines)
            sides = []
            for h in range(2):
                at = (2 * s + h) * quarter
                sides += [total[rows, at : at + quarter], expert_out[rows, at : at + quarter]]
            mixed = jnp.dot(spread, jnp.concatenate(sides, axis=0), preferred_element_type=F32)
            obuf[s, g * held : (g + 1) * held] = mixed.reshape(held, -1, quarter).astype(BF)
        stores.append(pltpu.make_async_copy(obuf.at[s], out.at[:, s], osems.at[s]))
        stores[s].start()
    for copy in stores:
        copy.wait()


def final_kernel(
    picks_h, returned, own_h, weight_h, route_h, out, picks, own, weight, route_w, sems
):
    loads = start_all(
        [(own_h, own), (weight_h, weight), (route_h, route_w), (picks_h, picks)], sems
    )
    for copy in loads:
        copy.wait()
    sums = jnp.dot(picks[...], returned[...], preferred_element_type=F32)
    seqs, quarter = own.shape[0], returned.shape[1]
    for h in range(2):
        dense, first, second = (
            sums[(2 * k + h) * seqs : (2 * k + h + 1) * seqs] for k in range(3)
        )
        cols = slice(h * quarter, (h + 1) * quarter)
        total = own[:, cols].astype(F32) + (route_w[:, :1] * first + route_w[:, 1:2] * second)
        out[:, cols] = (total + weight[:, :1] * dense).astype(BF)


def local(
    tokens,
    mix_gain,
    w_query,
    w_key,
    w_value,
    w_outgate,
    w_ingate,
    w_forget,
    in_bias,
    forget_bias,
    w_mix_out,
    cell_state,
    norm_state,
    max_state,
    moe_gain,
    route_ids,
    route_weights,
    expert_gate,
    expert_up,
    expert_down,
    branch_gate,
    dense_gate,
    dense_up,
    dense_down,
):
    seqs, width = tokens.shape
    tp_count = lax.axis_size("x")
    chips = lax.axis_size("q")
    ep_count = chips * CORES
    place = lax.axis_index("x")
    cols = width // tp_count
    half = width // 2
    head_count, hd = cell_state.shape[1:3]
    pair_rows = seqs * head_count
    groups = tp_count * CORES
    share = seqs // groups
    capacity = max(2, 4 * seqs // ep_count)
    swap = [(0, 1), (1, 0)]

    right = [(i, (i + 1) % tp_count) for i in range(tp_count)]
    left = [(i, (i - 1) % tp_count) for i in range(tp_count)]
    across = [(i, (i + 2) % tp_count) for i in range(tp_count)]

    top_count = route_ids.shape[1]
    chunk_rows = 2 * (share + capacity)
    total_rows = ep_count * chunk_rows
    pack = jnp.concatenate([dense_gate.T, dense_up.T, dense_down], axis=0)
    units = dense_down.shape[0]
    front_bytes = w_query.size * 4 * 2 + cell_state.size * 4
    (
        heads, carry, written, value, new_norm, new_max, slots, select, w_mix, tok, gain,
    ) = pl.pallas_call(
        front_kernel,
        in_specs=[SMEM] + [ANY] * 16,
        out_specs=[VMEM] + [ANY] * 6 + [VMEM] * 4,
        out_shape=[
            pltpu.VMEM((seqs, head_count * hd), BF),
            pltpu.HBM((pair_rows, hd), F32),
            pltpu.HBM((pair_rows, hd), F32),
            pltpu.HBM((pair_rows, hd), F32),
            pltpu.HBM((pair_rows, hd), F32),
            pltpu.HBM((head_count, seqs), F32),
            pltpu.HBM((seqs, 128), jnp.int32),
            pltpu.VMEM((total_rows, 128), BF),
            pltpu.VMEM(w_mix_out.shape, BF),
            pltpu.VMEM(tokens.shape, BF),
            pltpu.VMEM((1, width), F32),
        ],
        scratch_shapes=[
            pltpu.VMEM((top_count, seqs), jnp.int32),
            pltpu.VMEM((seqs, 128), jnp.int32),
            pltpu.VMEM((1, width), F32),
            pltpu.VMEM((head_count, width), BF),
            pltpu.VMEM((head_count, width), BF),
            pltpu.SMEM((head_count,), F32),
            pltpu.SMEM((head_count,), F32),
            pltpu.VMEM((pair_rows, hd), F32),
            pltpu.VMEM((head_count, seqs), F32),
            pltpu.VMEM((4, *w_query.shape), BF),
            pltpu.VMEM(cell_state.shape, F32),
            pltpu.VMEM((head_count, seqs, hd), F32),
            pltpu.VMEM((pair_rows, hd), F32),
            pltpu.VMEM((pair_rows, hd), F32),
            pltpu.VMEM((pair_rows, hd), F32),
            pltpu.VMEM((pair_rows, hd), F32),
            pltpu.VMEM((head_count, seqs), F32),
            pltpu.VMEM((128, seqs * hd), BF),
            pltpu.SemaphoreType.DMA((10,)),
            pltpu.SemaphoreType.DMA((5,)),
            pltpu.SemaphoreType.DMA((6,)),
            pltpu.SemaphoreType.DMA((6,)),
        ],
        compiler_params=params(40),
        cost_estimate=pl.CostEstimate(
            flops=2 * seqs * width * 4 * head_count * hd, transcendentals=0, bytes_accessed=front_bytes
        ),
        name="front",
    )(place.reshape(1), *(far_memory(a) for a in (
        route_ids.T,
        tokens,
        mix_gain.reshape(1, width),
        w_ingate.T,
        w_forget.T,
        in_bias,
        forget_bias,
        norm_state.reshape(pair_rows, hd),
        max_state.T,
        w_query,
        w_key,
        w_value,
        w_outgate,
        cell_state,
        w_mix_out,
        moe_gain.reshape(1, width),
    )))
    heads_l = lax.ppermute(heads, "x", right)
    heads_r = lax.ppermute(heads, "x", left)
    heads_f = lax.ppermute(heads, "x", across)
    out_way = right + [(tp_count + i, tp_count + j) for i, j in left]
    back_way = left + [(tp_count + i, tp_count + j) for i, j in right]
    pack_1 = lax.ppermute(pack, ("c", "x"), out_way)
    pack_2 = lax.ppermute(pack, ("c", "x"), back_way)
    pack_3 = lax.ppermute(pack_1, ("c", "x"), out_way)
    packs = [pack, pack_1, pack_2, pack_3]
    packs += [lax.ppermute(w, "c", swap) for w in packs]

    send, own, moe_in = pl.pallas_call(
        mix_kernel,
        in_specs=[SMEM] + [VMEM] * 8,
        out_specs=[ANY] * 3,
        out_shape=[
            pltpu.HBM((total_rows, half), BF),
            pltpu.HBM((seqs, cols), BF),
            pltpu.HBM((seqs, width), BF),
        ],
        scratch_shapes=[
            pltpu.VMEM((total_rows, half), BF),
            pltpu.VMEM((seqs, cols), BF),
            pltpu.VMEM((seqs, width), BF),
            pltpu.SemaphoreType.DMA((6,)),
        ],
        compiler_params=params(30),
        cost_estimate=pl.CostEstimate(
            flops=2 * seqs * width * w_mix_out.shape[0], transcendentals=0, bytes_accessed=w_mix_out.size * 2
        ),
        name="mix",
    )(
        place.reshape(1),
        *(near_memory(a) for a in (heads, heads_l, heads_r, heads_f, w_mix, tok, gain, select)),
    )
    arrived = lax.all_to_all(
        send.reshape(ep_count, chunk_rows, half), EP, split_axis=0, concat_axis=0, tiled=True
    )
    sources = ep_count * tp_count
    quarter = cols // 2
    picks, weight = pl.pallas_call(
        plan_kernel,
        in_specs=[VMEM] * 3,
        out_specs=[VMEM] * 2,
        out_shape=[
            pltpu.HBM((6 * seqs, sources * chunk_rows), BF),
            pltpu.HBM((seqs, 128), F32),
        ],
        compiler_params=params(),
        name="plan",
    )(slots, moe_in, branch_gate.reshape(1, width))
    many = ep_count * share
    back = pl.pallas_call(
        ffn_kernel,
        in_specs=[VMEM] + [ANY] * 11,
        out_specs=ANY,
        out_shape=pltpu.HBM((ep_count, tp_count, chunk_rows, quarter), BF),
        scratch_shapes=[
            pltpu.VMEM(expert_gate.shape, BF),
            pltpu.VMEM(expert_up.shape, BF),
            pltpu.VMEM(expert_down.shape, BF),
            pltpu.VMEM((8 * units, width), BF),
            pltpu.VMEM((8 * units, width), BF),
            pltpu.VMEM((8 * units, width), BF),
            pltpu.VMEM((2, many, width), BF),
            pltpu.VMEM((tp_count, ep_count, chunk_rows, quarter), BF),
            pltpu.SemaphoreType.DMA((27,)),
            pltpu.SemaphoreType.DMA((tp_count,)),
        ],
        compiler_params=params(46),
        cost_estimate=pl.CostEstimate(
            flops=6 * many * width * (8 * units + expert_down.shape[1]),
            transcendentals=0,
            bytes_accessed=6 * width * (8 * units + expert_down.shape[1]),
        ),
        name="ffn",
    )(near_memory(arrived.reshape(total_rows, half)), *(far_memory(a) for a in (
        expert_gate, expert_up, expert_down,
        *packs,
    )))
    returned = lax.all_to_all(
        back.reshape(sources, chunk_rows, quarter), ALL, split_axis=0, concat_axis=0, tiled=True
    )
    pairs = 16
    flat = pl.BlockSpec((pairs, hd), lambda i: (i, 0))
    cube = pl.BlockSpec((pairs, hd, hd), lambda i: (i, 0, 0))
    new_cell = pl.pallas_call(
        update_kernel,
        grid=(pair_rows // pairs,),
        in_specs=[flat, flat, flat, cube],
        out_specs=cube,
        out_shape=pltpu.HBM((pair_rows, hd, hd), F32),
        compiler_params=params(),
        cost_estimate=pl.CostEstimate(
            flops=3 * cell_state.size, transcendentals=0, bytes_accessed=8 * cell_state.size
        ),
        name="update",
    )(carry, written, value, far_memory(cell_state.reshape(pair_rows, hd, hd)))
    layer_out = pl.pallas_call(
        final_kernel,
        in_specs=[ANY, VMEM, ANY, ANY, ANY],
        out_specs=VMEM,
        out_shape=pltpu.HBM((seqs, cols), BF),
        scratch_shapes=[
            pltpu.VMEM((6 * seqs, sources * chunk_rows), BF),
            pltpu.VMEM((seqs, cols), BF),
            pltpu.VMEM((seqs, 128), F32),
            pltpu.VMEM(route_weights.shape, F32),
            pltpu.SemaphoreType.DMA((4,)),
        ],
        compiler_params=params(40),
        name="final",
    )(
        far_memory(picks),
        near_memory(returned.reshape(sources * chunk_rows, quarter)),
        *(far_memory(a) for a in (own, weight, route_weights)),
    )
    return (
        layer_out,
        new_cell.reshape(cell_state.shape),
        new_norm.reshape(norm_state.shape),
        new_max.T,
    )


def solution(mesh):
    ep_count, tp_count = mesh.shape["ep"], mesh.shape["tp"]
    mesh = Mesh(mesh.devices.reshape(ep_count // CORES, CORES, tp_count), ALL)
    in_specs = (
        P(EP, None),
        P(),
        P(None, "x"),
        P(None, "x"),
        P(None, "x"),
        P(None, "x"),
        P(None, "x"),
        P(None, "x"),
        P("x"),
        P("x"),
        P(),
        P(EP, "x", None, None),
        P(EP, "x", None),
        P(EP, "x"),
        P(),
        P(EP, None),
        P(EP, None),
        P(EP, None, "x"),
        P(EP, None, "x"),
        P(EP, "x", None),
        P(),
        P(None, ALL),
        P(None, ALL),
        P(ALL, None),
    )
    out_specs = (P(EP, "x"), P(EP, "x", None, None), P(EP, "x", None), P(EP, "x"))
    return jax.shard_map(local, mesh=mesh, in_specs=in_specs, out_specs=out_specs, check_vma=False)
```
